32 devices in a mesh: ep: 16 (over z, y, x), tp: 2 (over core).
Axes of the slice: x: 2, y: 2, z: 4, core: 2. Of those that a mesh axis runs over, the one named last changes fastest.
Arguments:
- tokens: bfloat16 [32, 2048], P('ep'), may hold values from -6 to 6
- head_state: float32 [32, 32, 64, 128], P('ep', 'tp'), may hold values from -4 to 4
- conv_state: bfloat16 [32, 3, 2048], P('ep', None, 'tp'), may hold values from -6 to 6
- conv_proj_state: bfloat16 [32, 3, 2, 512], P('ep', None, None, 'tp'), may hold values from -6 to 6
- first_gain: float32 [2048], replicated, may hold values from 0.1 to 1.9
- gate_weight: bfloat16 [2048, 2048], P('ep', 'tp'), may hold values from -0.125 to 0.125
- inner_weight: bfloat16 [2048, 2048], P('ep', 'tp'), may hold values from -0.125 to 0.125
- write_weight: bfloat16 [2048, 512], P(None, 'tp'), may hold values from -0.125 to 0.125
- read_weight: bfloat16 [2048, 512], P(None, 'tp'), may hold values from -0.125 to 0.125
- step_weight: bfloat16 [2048, 32], P(None, 'tp'), may hold values from -0.125 to 0.125
- conv_kernel: float32 [4, 2048], P(None, 'tp'), may hold values from -3 to 3
- conv_proj_kernel: float32 [4, 2, 512], P(None, None, 'tp'), may hold values from -3 to 3
- step_bias: float32 [32], P('tp'), may hold values from -2 to 1
- log_rate: float32 [32], P('tp'), may hold values from -4.5 to 1.5
- skip_gain: float32 [32], P('tp'), may hold values from 0.5 to 2
- group_gain: float32 [2048], P('tp'), may hold values from 0.1 to 1.9
- out_weight: bfloat16 [2048, 2048], P('tp', 'ep'), may hold values from -0.125 to 0.125
- second_gain: float32 [2048], replicated, may hold values from 0.1 to 1.9
- routes: int32 [32, 4], P('ep'), may hold values from 0 to 15, all different within a row; in each aligned block of 32 rows (0 to 31, 32 to 63, ...) at most 32 rows name the same one
- route_logits: bfloat16 [32, 4], P('ep'), may hold values from -8 to 300
- expert_gate: bfloat16 [16, 2048, 1024], P('ep', None, 'tp'), may hold values from -0.5 to 0.5
- expert_up: bfloat16 [16, 2048, 1024], P('ep', None, 'tp'), may hold values from -0.5 to 0.5
- expert_down: bfloat16 [16, 1024, 2048], P('ep', 'tp'), may hold values from -0.0234375 to 0.0234375
- dense_up: bfloat16 [2048, 4096], P(None, ('ep', 'tp')), may hold values from -0.125 to 0.125
- dense_down: bfloat16 [4096, 2048], P(('ep', 'tp')), may hold values from -0.09375 to 0.09375
- dense_gate: float32 [2048], replicated, may hold values from -0.125 to 0.125
Outputs:
- layer_out: bfloat16 [32, 2048], P(('ep', 'tp'))
- state_out: float32 [32, 32, 64, 128], P('ep', 'tp')
- conv_out: bfloat16 [32, 3, 2048], P('ep', None, 'tp')
- conv_proj_out: bfloat16 [32, 3, 2, 512], P('ep', None, None, 'tp')
The draws below stay inside these ranges and needn't reach their ends.
Inputs may be any that keep to these rules, and one draw needn't show every extreme that they name: `routes`: each token names 4 different experts; over the whole batch no expert is named by more than 32 rows, a bound that some block reaches.
All inputs are finite; a program needn't handle non-finite values.
Results may differ from the reference program's by a relative error of at most 0.015.
Values may be sent and summed in bfloat16 or wider, within the bound.
A program may use at most 64 MiB of HBM per device.

```python
import math
import jax
import jax.numpy as jnp
import numpy as np
from jax import lax

D = 2048
HEADS = 32
HEAD_DIM = 64
STATE = 128
GROUPS = 4
KCONV = 4
DE = 1024
FD = 4096
TOPK = 4
INNER = 2048
GS = 512
EXPERTS = 16
TOKENS = 32
CAPACITY = 32


def draw_log_rate(key, part):
    return jax.random.uniform(key, (HEADS,), jnp.float32, -3.5, 1.5)


def draw_route_logits(key, part):
    base_key = jax.random.fold_in(key, 11)
    values = jnp.clip(1.5 * jax.random.normal(base_key, (TOKENS, TOPK), jnp.float32), -6.0, 6.0)
    return values.astype(jnp.bfloat16)


def steps_of(key, dims, split, low, high):
    level = 1.0
    for axis_at, parts in split:
        heights = jax.random.uniform(jax.random.fold_in(jax.random.fold_in(key, 6), axis_at), (parts,), jnp.float32, low / len(split), high / len(split))
        level = level * jnp.repeat(jnp.exp(heights), dims[axis_at] // parts).reshape((-1,) + (1,) * (len(dims) - 1 - axis_at))
    return level


def deal_out(stream_key, own, number, rows, amount, top, bound, slope):
    order = jax.random.permutation(stream_key, amount)
    packed, common = shares(amount, rows * top, bound, slope, True), shares(amount, rows * top, bound, slope, False)
    places = jnp.arange(amount)

    def named(sizes, rotation):
        used = int((sizes > 0).sum())
        fixed = max(1, used // 4)
        moved = fixed + (places - fixed + rotation * (used - fixed)) % max(1, amount - fixed)
        return jnp.zeros((amount,), jnp.int32).at[order[jnp.where(places < fixed, places, moved)]].set(jnp.asarray(sizes, jnp.int32))

    sizes = jnp.where(number % 4 == 0, named(packed, number // 4), named(common, number - number // 4 - 1))
    mixed = jax.random.permutation(jax.random.fold_in(own, 3), amount)
    giver, taker = mixed[0:amount // 2 * 2:2], mixed[1:amount // 2 * 2:2]
    room = jnp.minimum(sizes[giver] - 1, bound - sizes[taker]) // 2
    room = jnp.where((giver == order[0]) | (taker == order[0]) | (sizes[taker] == 0), 0, jnp.maximum(room, 0))
    moved = jax.random.randint(jax.random.fold_in(own, 4), (amount // 2,), 0, 1 << 20) % (room + 1)
    sizes = sizes.at[giver].add(-moved).at[taker].add(moved)
    items = jnp.searchsorted(jnp.cumsum(sizes), jnp.arange(rows * top), side="right").astype(jnp.int32)
    grid = items.reshape(top, rows).T
    grid = grid[jax.random.permutation(jax.random.fold_in(own, 1), rows)]
    rotation = jax.random.randint(jax.random.fold_in(own, 2), (rows, 1), 0, top)
    return jnp.take_along_axis(grid, (jnp.arange(top)[None, :] + rotation) % top, axis=1)


def shares(count, total, bound, skew, full):
    weights = [(1 << 20) // math.isqrt(rank ** skew) + 1 for rank in range(1, count + 1)]
    largest = bound if full else min(bound, max(-(-total // count), total * weights[0] // sum(weights)))
    least = 1 if total - largest >= count - 1 else 0
    holding, rest = [largest] + [least] * (count - 1), total - largest - least * (count - 1)
    while rest > 0:
        free = [i for i in range(1, count) if holding[i] < largest] or [i for i in range(1, count) if holding[i] < bound]
        mass, remaining = sum([weights[i] for i in free]), rest
        for i in free:
            addition = min(bound - holding[i], max(1, remaining * weights[i] // mass), rest)
            holding[i] = holding[i] + addition
            rest = rest - addition
    return np.array(holding)


def centred(key, extent, width, limit, cuts=(), kind=jnp.bfloat16):
    array = jax.random.normal(key, extent, jnp.float32) * width
    if len(cuts) > 0:
        array = steps_of(key, extent, cuts, -0.22, 0.18) * array
    return jnp.clip(array, min=-limit, max=limit).astype(kind)


def setup_inputs(seed: int = 0) -> dict:
    streams_of = jax.random.split(jax.random.key(seed), 27)
    tokens = centred(streams_of[0], (TOKENS, D), 1.0, 6.0, ((0, 16),))
    head_state = centred(streams_of[1], (TOKENS, HEADS, HEAD_DIM, STATE), 0.5, 4.0, ((0, 16), (1, 2)), jnp.float32)
    conv_state = centred(streams_of[2], (TOKENS, KCONV - 1, INNER), 1.0, 6.0, ((0, 16), (2, 2)))
    conv_proj_state = centred(streams_of[3], (TOKENS, KCONV - 1, 2, GS), 1.0, 6.0, ((0, 16), (3, 2)))
    first_gain = jnp.clip(1.0 + 0.18 * jax.random.normal(streams_of[4], (D,), jnp.float32), 0.1, 1.9)
    gate_weight = centred(streams_of[5], (D, INNER), D ** -0.5, 0.125, ((0, 16), (1, 2)))
    inner_weight = centred(streams_of[6], (D, INNER), D ** -0.5, 0.125, ((0, 16), (1, 2)))
    write_weight = centred(streams_of[7], (D, GS), D ** -0.5, 0.125, ((1, 2),))
    read_weight = centred(streams_of[8], (D, GS), D ** -0.5, 0.125, ((1, 2),))
    step_weight = centred(streams_of[9], (D, HEADS), D ** -0.5, 0.125, ((1, 2),))
    conv_kernel = centred(streams_of[10], (KCONV, INNER), 0.5, 3.0, ((1, 2),), jnp.float32)
    conv_proj_kernel = centred(streams_of[11], (KCONV, 2, GS), 0.5, 3.0, ((2, 2),), jnp.float32)
    step_bias = jnp.clip(-2.0 + 3.0 * jax.random.uniform(streams_of[12], (HEADS,), jnp.float32) ** steps_of(streams_of[12], (HEADS,), ((0, 2),), -0.2, 0.2), -2.0, 1.0)
    log_rate = draw_log_rate(jax.random.fold_in(streams_of[26], 71), 0)
    skip_gain = jnp.clip(0.5 + 1.5 * jax.random.uniform(streams_of[14], (HEADS,), jnp.float32) ** steps_of(streams_of[14], (HEADS,), ((0, 2),), -0.2, 0.2), 0.5, 2.0)
    group_gain = jnp.clip(1.0 + 0.18 * jax.random.normal(streams_of[15], (INNER,), jnp.float32), 0.1, 1.9)
    out_weight = centred(streams_of[16], (INNER, D), INNER ** -0.5, 0.125, ((0, 2), (1, 16)))
    second_gain = jnp.clip(1.0 + 0.18 * jax.random.normal(streams_of[17], (D,), jnp.float32), 0.1, 1.9)
    routes_keys = jax.random.split(jax.random.fold_in(streams_of[18], 1), TOKENS // TOKENS)
    routes_turns = jax.random.permutation(jax.random.fold_in(streams_of[18], 3), TOKENS // TOKENS)
    routes = jax.vmap(lambda own, number: deal_out(jax.random.fold_in(streams_of[18], 2), own, number, TOKENS, EXPERTS, TOPK, CAPACITY, 2))(routes_keys, routes_turns).reshape((TOKENS, TOPK))
    route_logits = draw_route_logits(jax.random.fold_in(streams_of[26], 71), 0)
    expert_gate = centred(streams_of[20], (EXPERTS, D, DE), (D // 16) ** -0.5, 0.5, ((0, 16), (2, 2)))
    expert_up = centred(streams_of[21], (EXPERTS, D, DE), (D // 16) ** -0.5, 0.5, ((0, 16), (2, 2)))
    expert_down = centred(streams_of[22], (EXPERTS, DE, D), (DE * 64) ** -0.5, 0.0234375, ((0, 16), (1, 2)))
    dense_up = centred(streams_of[23], (D, FD), D ** -0.5, 0.125, ((1, 32),))
    dense_down = centred(streams_of[24], (FD, D), FD ** -0.5, 0.09375, ((0, 32),))
    dense_gate = centred(streams_of[25], (D,), D ** -0.5, 0.125, (), jnp.float32)
    return dict(tokens=tokens, head_state=head_state, conv_state=conv_state, conv_proj_state=conv_proj_state, first_gain=first_gain, gate_weight=gate_weight, inner_weight=inner_weight, write_weight=write_weight, read_weight=read_weight, step_weight=step_weight, conv_kernel=conv_kernel, conv_proj_kernel=conv_proj_kernel, step_bias=step_bias, log_rate=log_rate, skip_gain=skip_gain, group_gain=group_gain, out_weight=out_weight, second_gain=second_gain, routes=routes, route_logits=route_logits, expert_gate=expert_gate, expert_up=expert_up, expert_down=expert_down, dense_up=dense_up, dense_down=dense_down, dense_gate=dense_gate)


norm_eps = 1e-05
clamp_limit = 7.0
glu_alpha = 1.702
highest = lax.Precision.HIGHEST

def rms_scale(values, gain_vec):
    return values * lax.rsqrt(lax.optimization_barrier(jnp.mean(values * values, axis=-1, keepdims=True)) + norm_eps) * gain_vec

def clamped_unit(gate_pre, up_pre):
    glu_part = jnp.minimum(gate_pre, clamp_limit)
    lin_part = jnp.clip(up_pre, -clamp_limit, clamp_limit)
    return glu_part * jax.nn.sigmoid(glu_alpha * glu_part) * (lin_part + 1.0)

def state_step(inner_proj, gate_proj, write_proj, read_proj, step_raw, conv_state, conv_proj_state, conv_kernel, conv_proj_kernel, step_bias, log_rate, skip_gain, group_gain, head_state, group_count):
    window_inner = jnp.concatenate([conv_state, inner_proj[:, None, :]], axis=1)
    window_proj = jnp.concatenate([conv_proj_state, jnp.stack([write_proj, read_proj], axis=1)[:, None]], axis=1)
    conv_inner = jax.nn.silu(lax.optimization_barrier(jnp.sum(window_inner.astype(jnp.float32) * conv_kernel[None], axis=1)))
    conv_proj = jax.nn.silu(lax.optimization_barrier(jnp.sum(window_proj.astype(jnp.float32) * conv_proj_kernel[None], axis=1)))
    seq_count, channels = conv_inner.shape
    head_count = step_raw.shape[1]
    head_width = channels // head_count
    state_width = conv_proj.shape[2] // group_count
    per_group = head_count // group_count
    head_input = conv_inner.reshape(seq_count, head_count, head_width)
    write_heads = jnp.repeat(conv_proj[:, 0].reshape(seq_count, group_count, state_width), per_group, axis=1)
    read_heads = jnp.repeat(conv_proj[:, 1].reshape(seq_count, group_count, state_width), per_group, axis=1)
    step_size = jax.nn.softplus(step_raw + step_bias)
    decay_rate = jnp.exp(-jnp.exp(log_rate) * step_size)
    state_out = decay_rate[:, :, None, None] * head_state + (step_size[:, :, None] * head_input)[:, :, :, None] * write_heads[:, :, None, :]
    read_out = jnp.einsum('shpn,shn->shp', state_out, read_heads, precision=highest) + skip_gain[None, :, None] * head_input
    gated_rows = read_out.reshape(seq_count, channels) * jax.nn.silu(gate_proj.astype(jnp.float32))
    grouped = gated_rows.reshape(seq_count, group_count, channels // group_count)
    grouped = grouped * lax.rsqrt(lax.optimization_barrier(jnp.mean(grouped * grouped, axis=-1, keepdims=True)) + norm_eps)
    mixer_rows = (grouped.reshape(seq_count, channels) * group_gain).astype(jnp.bfloat16)
    return (mixer_rows, state_out, window_inner[:, 1:], window_proj[:, 1:])

def reference(tokens, head_state, conv_state, conv_proj_state, first_gain, gate_weight, inner_weight, write_weight, read_weight, step_weight, conv_kernel, conv_proj_kernel, step_bias, log_rate, skip_gain, group_gain, out_weight, second_gain, routes, route_logits, expert_gate, expert_up, expert_down, dense_up, dense_down, dense_gate):
    normed_in = rms_scale(tokens.astype(jnp.float32), first_gain).astype(jnp.bfloat16)
    gate_proj = jnp.dot(normed_in, gate_weight, preferred_element_type=jnp.float32).astype(jnp.bfloat16)
    inner_proj = jnp.dot(normed_in, inner_weight, preferred_element_type=jnp.float32).astype(jnp.bfloat16)
    write_proj = jnp.dot(normed_in, write_weight, preferred_element_type=jnp.float32).astype(jnp.bfloat16)
    read_proj = jnp.dot(normed_in, read_weight, preferred_element_type=jnp.float32).astype(jnp.bfloat16)
    step_raw = jnp.dot(normed_in, step_weight, preferred_element_type=jnp.float32)
    mixer_rows, state_out, conv_out, conv_proj_out = state_step(inner_proj, gate_proj, write_proj, read_proj, step_raw, conv_state, conv_proj_state, conv_kernel, conv_proj_kernel, step_bias, log_rate, skip_gain, group_gain, head_state, GROUPS)
    mixed = jnp.dot(mixer_rows, out_weight, preferred_element_type=jnp.float32)
    hidden = (tokens.astype(jnp.float32) + mixed).astype(jnp.bfloat16)
    normed_mid = rms_scale(hidden.astype(jnp.float32), second_gain).astype(jnp.bfloat16)
    route_gates = jax.nn.softmax(route_logits.astype(jnp.float32), axis=-1)
    row_ids = jnp.arange(TOKENS, dtype=jnp.int32)

    def expert_pass(running, inputs):
        gate_block, up_block, down_block, expert_id = inputs
        route_hits = routes == expert_id
        row_weight = lax.optimization_barrier(jnp.sum(jnp.where(route_hits, route_gates, 0.0), axis=1))
        chosen = jnp.any(route_hits, axis=1)
        picked = jnp.argsort(jnp.where(chosen, row_ids, row_ids + TOKENS)).astype(jnp.int32)[:CAPACITY]
        picked_rows = normed_mid[picked]
        activated = clamped_unit(jnp.dot(picked_rows, gate_block, preferred_element_type=jnp.float32), jnp.dot(picked_rows, up_block, preferred_element_type=jnp.float32)).astype(jnp.bfloat16)
        expert_rows = jnp.dot(activated, down_block, preferred_element_type=jnp.float32) * row_weight[picked][:, None]
        return (running.at[picked].add(expert_rows), None)
    expert_ids = jnp.arange(EXPERTS, dtype=jnp.int32)
    expert_mix = lax.scan(expert_pass, jnp.zeros((TOKENS, D), jnp.float32), (expert_gate, expert_up, expert_down, expert_ids))[0]
    dense_act = jax.nn.silu(jnp.dot(normed_mid, dense_up, preferred_element_type=jnp.float32)).astype(jnp.bfloat16)
    dense_weight = jax.nn.sigmoid(jnp.dot(normed_mid.astype(jnp.float32), dense_gate, precision=highest))
    dense_value = jnp.dot(dense_act, dense_down, preferred_element_type=jnp.float32)
    layer_out = (hidden.astype(jnp.float32) + expert_mix + dense_weight[:, None] * dense_value).astype(jnp.bfloat16)
    return (layer_out, state_out, conv_out, conv_proj_out)
```

```python
import functools
import types

import jax
import jax.numpy as jnp
from jax import lax
from jax.experimental import pallas as pl
from jax.experimental.pallas import tpu as pltpu
from jax.sharding import PartitionSpec as P

GROUPS = 4


norm_eps = 1e-05
clamp_limit = 7.0
glu_alpha = 1.702
highest = lax.Precision.HIGHEST


def rms_scale(values, gain_vec):
    return (
        values * lax.rsqrt(jnp.mean(values * values, axis=-1, keepdims=True) + norm_eps) * gain_vec
    )


def clamped_unit(gate_pre, up_pre):
    glu_part = jnp.minimum(gate_pre, clamp_limit)
    lin_part = jnp.clip(up_pre, -clamp_limit, clamp_limit)
    return glu_part * jax.nn.sigmoid(glu_alpha * glu_part) * (lin_part + 1.0)


def state_step(
    inner_proj,
    gate_proj,
    write_proj,
    read_proj,
    step_raw,
    conv_state,
    conv_proj_state,
    conv_kernel,
    conv_proj_kernel,
    step_bias,
    log_rate,
    skip_gain,
    group_gain,
    head_state,
    group_count,
):
    window_inner = jnp.concatenate([conv_state, inner_proj[:, None, :]], axis=1)
    window_proj = jnp.concatenate(
        [conv_proj_state, jnp.stack([write_proj, read_proj], axis=1)[:, None]], axis=1
    )
    conv_inner = jax.nn.silu(jnp.sum(window_inner.astype(jnp.float32) * conv_kernel[None], axis=1))
    conv_proj = jax.nn.silu(
        jnp.sum(window_proj.astype(jnp.float32) * conv_proj_kernel[None], axis=1)
    )
    seq_count, channels = conv_inner.shape
    head_count = step_raw.shape[1]
    head_width = channels // head_count
    state_width = conv_proj.shape[2] // group_count
    per_group = head_count // group_count
    head_input = conv_inner.reshape(seq_count, head_count, head_width)
    write_heads = jnp.repeat(
        conv_proj[:, 0].reshape(seq_count, group_count, state_width), per_group, axis=1
    )
    read_heads = jnp.repeat(
        conv_proj[:, 1].reshape(seq_count, group_count, state_width), per_group, axis=1
    )
    step_size = jax.nn.softplus(step_raw + step_bias)
    decay_rate = jnp.exp(-jnp.exp(log_rate) * step_size)
    state_out = (
        decay_rate[:, :, None, None] * head_state
        + (step_size[:, :, None] * head_input)[:, :, :, None] * write_heads[:, :, None, :]
    )
    read_out = (
        jnp.einsum("shpn,shn->shp", state_out, read_heads, precision=highest)
        + skip_gain[None, :, None] * head_input
    )
    gated_rows = read_out.reshape(seq_count, channels) * jax.nn.silu(gate_proj.astype(jnp.float32))
    grouped = gated_rows.reshape(seq_count, group_count, channels // group_count)
    grouped = grouped * lax.rsqrt(jnp.mean(grouped * grouped, axis=-1, keepdims=True) + norm_eps)
    mixer_rows = (grouped.reshape(seq_count, channels) * group_gain).astype(jnp.bfloat16)
    return (mixer_rows, state_out, window_inner[:, 1:], window_proj[:, 1:])


def local(
    tokens,
    head_state,
    conv_state,
    conv_proj_state,
    first_gain,
    gate_weight,
    inner_weight,
    write_weight,
    read_weight,
    step_weight,
    conv_kernel,
    conv_proj_kernel,
    step_bias,
    log_rate,
    skip_gain,
    group_gain,
    out_weight,
    second_gain,
    routes,
    route_logits,
    expert_gate,
    expert_up,
    expert_down,
    dense_up,
    dense_down,
    dense_gate,
):
    seq_count = tokens.shape[0]
    half_width = gate_weight.shape[1]
    normed_in = rms_scale(tokens.astype(jnp.float32), first_gain).astype(jnp.bfloat16)
    features = lax.all_to_all(normed_in, "ep", split_axis=1, concat_axis=0, tiled=True)
    row_block = features
    both_terms = lax.psum_scatter(
        jnp.concatenate(
            [
                jnp.dot(row_block, gate_weight, preferred_element_type=jnp.float32),
                jnp.dot(row_block, inner_weight, preferred_element_type=jnp.float32),
            ],
            axis=1,
        ),
        "ep",
        scatter_dimension=0,
        tiled=True,
    )
    gate_sum = both_terms[:, :half_width]
    inner_sum = both_terms[:, half_width:]
    gate_proj = gate_sum.astype(jnp.bfloat16)
    inner_proj = inner_sum.astype(jnp.bfloat16)
    write_proj = jnp.dot(normed_in, write_weight, preferred_element_type=jnp.float32).astype(
        jnp.bfloat16
    )
    read_proj = jnp.dot(normed_in, read_weight, preferred_element_type=jnp.float32).astype(
        jnp.bfloat16
    )
    step_raw = jnp.dot(normed_in, step_weight, preferred_element_type=jnp.float32)
    local_groups = GROUPS // lax.axis_size("tp")
    mixer_rows, state_out, conv_out, conv_proj_out = state_step(
        inner_proj,
        gate_proj,
        write_proj,
        read_proj,
        step_raw,
        conv_state,
        conv_proj_state,
        conv_kernel,
        conv_proj_kernel,
        step_bias,
        log_rate,
        skip_gain,
        group_gain,
        head_state,
        local_groups,
    )
    partial_mix = jnp.dot(
        mixer_rows,
        lax.all_gather(out_weight, "ep", axis=1, tiled=True),
        preferred_element_type=jnp.float32,
    )
    mixed = lax.psum(partial_mix, "tp")
    hidden = (tokens.astype(jnp.float32) + mixed).astype(jnp.bfloat16)
    normed_mid = rms_scale(hidden.astype(jnp.float32), second_gain).astype(jnp.bfloat16)
    all_rows, all_routes, all_logits = (
        lax.all_gather(normed_mid, "ep", axis=0, tiled=True),
        lax.all_gather(routes, "ep", axis=0, tiled=True),
        lax.all_gather(route_logits, "ep", axis=0, tiled=True),
    )
    route_gates = jax.nn.softmax(all_logits.astype(jnp.float32), axis=-1)
    my_expert = lax.axis_index("ep")
    route_hits = all_routes == my_expert
    row_weight = jnp.sum(jnp.where(route_hits, route_gates, 0.0), axis=1)
    chosen = jnp.any(route_hits, axis=1)
    slot_index = jnp.cumsum(chosen.astype(jnp.int32)) - 1
    capacity = 4 * seq_count * routes.shape[1]
    slot_ids = jnp.arange(capacity, dtype=jnp.int32)
    picks = (slot_index[None, :] == slot_ids[:, None]) & chosen[None, :]
    picked_rows = jnp.dot(
        picks.astype(jnp.bfloat16), all_rows, preferred_element_type=jnp.float32
    ).astype(jnp.bfloat16)
    activated = clamped_unit(
        jnp.dot(picked_rows, expert_gate[0], preferred_element_type=jnp.float32),
        jnp.dot(picked_rows, expert_up[0], preferred_element_type=jnp.float32),
    ).astype(jnp.bfloat16)
    expert_part = jnp.dot(activated, expert_down[0], preferred_element_type=jnp.float32)
    placed = jnp.where(picks, row_weight[None, :], 0.0)
    dense_weight = jax.nn.sigmoid(
        jnp.dot(all_rows.astype(jnp.float32), dense_gate, precision=highest)
    )
    row_share = seq_count // lax.axis_size("tp")
    row_block = all_rows
    dense_inner = jax.nn.silu(
        jnp.dot(row_block, dense_up, preferred_element_type=jnp.float32)
    ).astype(jnp.bfloat16)
    dense_term = (
        jnp.dot(dense_inner, dense_down, preferred_element_type=jnp.float32) * dense_weight[:, None]
    )
    summed = lax.psum_scatter(
        dense_term + jnp.einsum("cr,cd->rd", placed, expert_part, precision=highest),
        ("ep", "tp"),
        scatter_dimension=0,
        tiled=True,
    )
    own_rows = lax.dynamic_slice_in_dim(hidden, lax.axis_index("tp") * row_share, row_share, 0)
    layer_out = (own_rows.astype(jnp.float32) + summed).astype(jnp.bfloat16)
    return (layer_out, state_out, conv_out, conv_proj_out)


LANES = 128
MESH = pl.DeviceIdType.MESH
F32 = jnp.float32
BF16 = jnp.bfloat16


def silu(x):
    return x * jax.nn.sigmoid(x)


def dot(a, b):
    return jnp.dot(a, b, preferred_element_type=F32)


def lanes_of(ref, start, count, stride, pieces):
    return jnp.concatenate(
        [ref[pl.ds(start + j, count, stride=stride), :] for j in range(pieces)], axis=1
    )


def layer_kernel(
    n,
    nc,
    names,
    scratch_names,
    *refs,
):
    r = types.SimpleNamespace(**dict(zip(names + scratch_names, refs)))
    me = lax.axis_index("ep")
    core = lax.axis_index("tp")
    q = r.tokens.shape[0]
    width = r.tokens.shape[1]
    half = r.gate_v.shape[1]
    chunks = half // LANES
    wide_chunks = width // LANES
    rows = n * q
    slot1 = r.send1.shape[0] // n
    slot2 = 2 * q * chunks
    slot3 = q * chunks
    slot6 = wide_chunks
    heads = r.step_bias.shape[1]
    head_width = half // heads
    state_width = r.hs.shape[2]
    groups = r.write_v.shape[1] // state_width
    group_width = half // groups
    topk = r.routes.shape[1]

    barrier = pltpu.get_barrier_semaphore()

    def greet(step, _):
        other = lax.rem(me * nc + core + step, n * nc)
        pl.semaphore_signal(
            barrier, inc=1, device_id=(other // nc, lax.rem(other, nc)), device_id_type=MESH
        )
        return 0

    lax.fori_loop(1, n * nc, greet, 0)

    order = (
        (r.gate_weight, r.gate_v),
        (r.inner_weight, r.inner_v),
        (r.write_weight, r.write_v),
        (r.read_weight, r.read_v),
        (r.step_weight, r.step_v),
        (r.head_state, r.hs),
        (r.out_weight, r.out_v),
        (r.expert_gate, r.eg_v),
        (r.expert_up, r.eu_v),
        (r.dense_up, r.du_v),
        (r.expert_down, r.ed_v),
        (r.dense_down, r.dd_v),
    )
    loads = [
        pltpu.make_async_copy(src, dst, r.load_sem.at[i]) for i, (src, dst) in enumerate(order)
    ]
    for load in loads:
        load.start()
    (
        gate_load,
        inner_load,
        write_load,
        read_load,
        step_load,
        state_load,
        out_load,
        expert_gate_load,
        expert_up_load,
        dense_up_load,
        expert_down_load,
        dense_down_load,
    ) = loads

    def all_to_all(phase, send, recv, slot, same=False):
        def one(step, _):
            peer = lax.rem(me + step, n)
            src = send if same else send.at[pl.ds(pl.multiple_of(peer * slot, slot), slot)]
            pltpu.make_async_remote_copy(
                src_ref=src,
                dst_ref=recv.at[pl.ds(pl.multiple_of(me * slot, slot), slot)],
                send_sem=r.send_sem.at[phase],
                recv_sem=r.recv_sem.at[phase],
                device_id=(peer, core),
                device_id_type=MESH,
            ).start()
            return 0

        lax.fori_loop(1, n, one, 0)

    def drain(sem, buffer, count):
        part = buffer.at[pl.ds(0, count)]
        pltpu.make_async_copy(part, part, sem).wait()

    def take(phase, send, recv, slot, same=False):
        drain(r.recv_sem.at[phase], recv, (n - 1) * slot)
        mine = pl.ds(pl.multiple_of(me * slot, slot), slot)
        recv[mine, :] = send[...] if same else send[mine, :]

    x = r.tokens[...].astype(F32)
    normed = rms_scale(x, r.first_gain[...]).astype(BF16).astype(F32)
    send1 = r.send1
    send1[...] = jnp.zeros_like(send1)
    chosen = r.routes[...].astype(F32)
    scores = r.route_logits[...].astype(F32)
    for e in range(n):
        at, cut = e * slot1, slice(e * LANES, (e + 1) * LANES)
        send1[at : at + q, :] = normed[:, cut]
        send1[at + q : at + 2 * q, :] = x[:, cut]
        send1[at + 2 * q : at + 3 * q, 0:topk] = chosen
        send1[at + 3 * q : at + 4 * q, 0:topk] = scores
    pl.semaphore_wait(barrier, n * nc - 1)
    all_to_all(0, send1, r.recv1, slot1)

    own = r.own_rows
    own[...] = jnp.zeros_like(own)
    own[0:q, :] = normed
    own_b = own[...].astype(BF16)
    gate_load.wait()
    inner_load.wait()
    write_load.wait()
    read_load.wait()
    step_load.wait()
    write_proj = dot(own_b, r.write_v[...])[0:q].astype(BF16)
    read_proj = dot(own_b, r.read_v[...])[0:q].astype(BF16)
    step_raw = dot(own_b, r.step_v[...])[0:q]

    take(0, send1, r.recv1, slot1)
    recv1 = r.recv1

    def gathered(offset):
        return jnp.concatenate(
            [recv1[pl.ds(offset + s, n, stride=slot1), :] for s in range(q)], axis=0
        )

    features = gathered(0).astype(BF16)
    pack2 = r.pack2
    for g, weight in enumerate((r.gate_v, r.inner_v)):
        part = dot(features, weight[...])
        for s in range(q):
            for j in range(chunks):
                pack2[pl.ds((s * 2 + g) * chunks + j, n, stride=slot2), :] = part[
                    s * n : (s + 1) * n, j * LANES : (j + 1) * LANES
                ]
    r.send2[...] = pack2[...].astype(BF16)
    all_to_all(1, r.send2, r.recv2, slot2)

    r.proj_out[:, 0 : groups * state_width] = write_proj
    r.proj_out[:, groups * state_width :] = read_proj
    proj_tap = r.conv_proj_kernel[r.conv_proj_kernel.shape[0] - 1]
    gs = groups * state_width
    write = silu(r.proj_part[:, 0:gs] + write_proj.astype(F32) * proj_tap[0:1])
    read = silu(r.proj_part[:, gs:] + read_proj.astype(F32) * proj_tap[1:2])
    pre = step_raw + r.step_bias[...]
    step_size = jnp.maximum(pre, 0.0) + jnp.log1p(jnp.exp(-jnp.abs(pre)))
    decay = jnp.exp(-jnp.exp(r.log_rate[...]) * step_size)
    small = r.small
    small[...] = jnp.zeros_like(small)
    small[0:q, :] = step_size
    small[q : 2 * q, :] = decay
    small[2 * q : 2 * q + 1, :] = r.skip_gain[...]
    spread = (
        lax.broadcasted_iota(jnp.int32, (heads, half), 1) // head_width
        == lax.broadcasted_iota(jnp.int32, (heads, half), 0)
    ).astype(F32)
    by_channel = jnp.dot(small[...], spread, precision=highest, preferred_element_type=F32)
    step_rows, decay_rows = by_channel[0:q], by_channel[q : 2 * q]
    skip_rows = by_channel[2 * q : 2 * q + 1]
    reads = r.reads
    reads[...] = jnp.zeros_like(reads)
    reads[0:q, :] = read
    state_load.wait()
    old_read = r.old_read
    write_read = []
    for g in range(groups):
        lane = slice(g * state_width, (g + 1) * state_width)
        span = slice(g * group_width, (g + 1) * group_width)
        write_read.append(
            jnp.broadcast_to(
                jnp.sum(write[:, lane] * read[:, lane], axis=1, keepdims=True), (q, group_width)
            )
        )
        for s in range(q):
            old_read[s : s + 1, span] = lax.dot_general(
                reads[:, lane],
                r.hs[s, span, :],
                (((1,), (1,)), ((), ())),
                precision=highest,
                preferred_element_type=F32,
            )[s : s + 1]
    carried = decay_rows * old_read[0:q, :]
    direct = step_rows * jnp.concatenate(write_read, axis=1) + skip_rows

    all_routes, all_scores = gathered(2 * q), gathered(3 * q)
    real = lax.broadcasted_iota(jnp.int32, (rows, LANES), 1) < topk
    top = jnp.max(jnp.where(real, all_scores, -jnp.inf), axis=1, keepdims=True)
    raised = jnp.where(real, jnp.exp(jnp.where(real, all_scores - top, 0.0)), 0.0)
    gates = raised / jnp.sum(raised, axis=1, keepdims=True)
    hits = real & (all_routes == me.astype(F32))
    row_weight = jnp.sum(jnp.where(hits, gates, 0.0), axis=1, keepdims=True)

    take(1, r.send2, r.recv2, slot2)
    total = r.recv2[0:slot2, :].astype(F32)
    for e in range(1, n):
        total += r.recv2[e * slot2 : (e + 1) * slot2, :].astype(F32)
    r.sum2[...] = total
    gate_proj = lanes_of(r.sum2, 0, q, 2 * chunks, chunks).astype(BF16).astype(F32)
    inner_proj = lanes_of(r.sum2, chunks, q, 2 * chunks, chunks).astype(BF16)
    last_tap = r.conv_kernel.shape[0] - 1
    taps = r.conv_kernel[last_tap : last_tap + 1, :]
    conv_inner = silu(r.inner_part[...] + inner_proj.astype(F32) * taps)
    gated = (carried + direct * conv_inner) * silu(gate_proj)
    normal = []
    for g in range(groups):
        piece = gated[:, g * group_width : (g + 1) * group_width]
        normal.append(
            piece * lax.rsqrt(jnp.mean(piece * piece, axis=1, keepdims=True) + norm_eps)
        )
    mixer = jnp.concatenate(normal, axis=1) * r.group_gain[...]
    for j in range(chunks):
        r.pack3[pl.ds(j, q, stride=chunks), :] = mixer[:, j * LANES : (j + 1) * LANES]
    r.send3[...] = r.pack3[...].astype(BF16)
    all_to_all(2, r.send3, r.recv3, slot3, same=True)

    r.inner_out[...] = inner_proj
    turn = r.turn
    turn[...] = jnp.zeros_like(turn)
    turn[0:q, :] = decay_rows
    turn[q : 2 * q, :] = step_rows * conv_inner
    columns = jnp.transpose(turn[...])
    for s in range(q):
        for k in range(chunks):
            span = slice(k * LANES, (k + 1) * LANES)
            g = k * LANES // group_width
            r.hs[s, span, :] = (
                columns[span, s : s + 1] * r.hs[s, span, :]
                + columns[span, q + s : q + s + 1]
                * write[s : s + 1, g * state_width : (g + 1) * state_width]
            )
    store = pltpu.make_async_copy(r.hs, r.state_out, r.load_sem.at[len(order)])
    store.start()
    raw_block = gathered(q)
    out_load.wait()

    take(2, r.send3, r.recv3, slot3, same=True)
    r.wide3[...] = r.recv3[...].astype(F32)
    all_mixer = jnp.concatenate(
        [lanes_of(r.wide3, s * chunks, n, slot3, chunks) for s in range(q)], axis=0
    ).astype(BF16)
    part = dot(all_mixer, r.out_v[...])
    r.send4[...] = part
    swap = pltpu.make_async_remote_copy(
        src_ref=r.send4,
        dst_ref=r.recv4,
        send_sem=r.send_sem.at[3],
        recv_sem=r.recv_sem.at[3],
        device_id=(me, lax.rem(core + 1, nc)),
        device_id_type=MESH,
    )
    swap.start()
    swap.wait_recv()
    r.send5[...] = (raw_block + (part + r.recv4[...])).astype(BF16)
    all_to_all(4, r.send5, r.recv5, rows, same=True)
    expert_gate_load.wait()
    expert_up_load.wait()
    dense_up_load.wait()
    take(4, r.send5, r.recv5, rows, same=True)
    hidden = jnp.concatenate(
        [r.recv5[e * rows : (e + 1) * rows, :] for e in range(n)], axis=1
    ).astype(F32)
    r.hidden[...] = hidden
    mid = rms_scale(hidden, r.second_gain[...]).astype(BF16)
    dense_inner = silu(dot(mid, r.du_v[...])).astype(BF16)
    activated = clamped_unit(dot(mid, r.eg_v[...]), dot(mid, r.eu_v[...])).astype(BF16)
    dense_weight = jax.nn.sigmoid(
        jnp.sum(mid.astype(F32) * r.dense_gate[...], axis=1, keepdims=True)
    )
    expert_down_load.wait()
    dense_down_load.wait()
    cuts = 4
    for c in range(cuts):
        span = slice(c * width // cuts, (c + 1) * width // cuts)
        term = dot(activated, r.ed_v[:, span]) * row_weight
        term += dot(dense_inner, r.dd_v[:, span]) * dense_weight
        for j in range(wide_chunks // cuts):
            r.pack6[pl.ds(c * wide_chunks // cuts + j, rows, stride=slot6), :] = term[
                :, j * LANES : (j + 1) * LANES
            ]
    r.send6[...] = r.pack6[...].astype(BF16)
    mine = me * nc + core

    def one(step, _):
        other = lax.rem(mine + step, n * nc)
        peer, peer_core = other // nc, lax.rem(other, nc)
        pltpu.make_async_remote_copy(
            src_ref=r.send6.at[
                pl.ds(pl.multiple_of((peer_core * n + peer) * slot6, slot6), slot6)
            ],
            dst_ref=r.recv6.at[pl.ds(pl.multiple_of(mine * slot6, slot6), slot6)],
            send_sem=r.send_sem.at[5],
            recv_sem=r.recv_sem.at[5],
            device_id=(peer, peer_core),
            device_id_type=MESH,
        ).start()
        return 0

    lax.fori_loop(1, n * nc, one, 0)
    own_row = r.hidden[pl.ds(core * n + me, 1), :]
    drain(r.recv_sem.at[5], r.recv6, (n * nc - 1) * slot6)
    r.recv6[pl.ds(pl.multiple_of(mine * slot6, slot6), slot6), :] = r.send6[
        pl.ds(pl.multiple_of((core * n + me) * slot6, slot6), slot6), :
    ]
    total = r.recv6[0:slot6, :].astype(F32)
    for e in range(1, n * nc):
        total += r.recv6[e * slot6 : (e + 1) * slot6, :].astype(F32)
    r.sum6[...] = total
    summed = jnp.concatenate([r.sum6[j : j + 1, :] for j in range(wide_chunks)], axis=1)
    r.layer_out[...] = (own_row + summed).astype(BF16)

    store.wait()
    drain(r.send_sem.at[0], send1, (n - 1) * slot1)
    drain(r.send_sem.at[1], r.send2, (n - 1) * slot2)
    drain(r.send_sem.at[2], r.recv3, (n - 1) * slot3)
    swap.wait_send()
    drain(r.send_sem.at[4], r.recv5, (n - 1) * rows)
    drain(r.send_sem.at[5], r.send6, (n * nc - 1) * slot6)


def fused_local(
    n,
    nc,
    tokens,
    head_state,
    conv_state,
    conv_proj_state,
    first_gain,
    gate_weight,
    inner_weight,
    write_weight,
    read_weight,
    step_weight,
    conv_kernel,
    conv_proj_kernel,
    step_bias,
    log_rate,
    skip_gain,
    group_gain,
    out_weight,
    second_gain,
    routes,
    route_logits,
    expert_gate,
    expert_up,
    expert_down,
    dense_up,
    dense_down,
    dense_gate,
):
    q, width = tokens.shape
    half = gate_weight.shape[1]
    rows = n * q
    chunks, wide_chunks = half // LANES, width // LANES
    gs = write_weight.shape[1]
    heads, state_width = head_state.shape[1], head_state.shape[3]
    taps = conv_kernel.shape[0]
    inner_part = jnp.sum(conv_state.astype(F32) * conv_kernel[None, : taps - 1], axis=1)
    proj_part = jnp.sum(
        conv_proj_state.astype(F32) * conv_proj_kernel[None, : taps - 1], axis=1
    ).reshape(q, 2 * gs)
    small_in = dict(
        tokens=tokens,
        first_gain=first_gain[None],
        inner_part=inner_part,
        proj_part=proj_part,
        conv_kernel=conv_kernel,
        conv_proj_kernel=conv_proj_kernel,
        step_bias=step_bias[None],
        log_rate=log_rate[None],
        skip_gain=skip_gain[None],
        group_gain=group_gain[None],
        second_gain=second_gain[None],
        routes=routes,
        route_logits=route_logits,
        dense_gate=dense_gate[None],
    )
    big_in = dict(
        head_state=head_state.reshape(q, half, state_width),
        gate_weight=gate_weight,
        inner_weight=inner_weight,
        write_weight=write_weight,
        read_weight=read_weight,
        step_weight=step_weight,
        out_weight=out_weight,
        expert_gate=expert_gate[0],
        expert_up=expert_up[0],
        expert_down=expert_down[0],
        dense_up=dense_up,
        dense_down=dense_down,
    )
    outs = dict(
        layer_out=jax.ShapeDtypeStruct((q // nc, width), BF16),
        state_out=jax.ShapeDtypeStruct((q, half, state_width), F32),
        inner_out=jax.ShapeDtypeStruct((q, half), BF16),
        proj_out=jax.ShapeDtypeStruct((q, 2 * gs), BF16),
    )
    slot1 = -(-4 * q // 8) * 8
    slot2, slot3, slot6 = 2 * q * chunks, q * chunks, wide_chunks
    small_rows = -(-(2 * q + 1) // 8) * 8
    vmem = pltpu.VMEM
    scratch = dict(
        gate_v=vmem(gate_weight.shape, BF16),
        inner_v=vmem(inner_weight.shape, BF16),
        write_v=vmem(write_weight.shape, BF16),
        read_v=vmem(read_weight.shape, BF16),
        step_v=vmem(step_weight.shape, BF16),
        hs=vmem((q, half, state_width), F32),
        out_v=vmem(out_weight.shape, BF16),
        eg_v=vmem(expert_gate.shape[1:], BF16),
        eu_v=vmem(expert_up.shape[1:], BF16),
        du_v=vmem(dense_up.shape, BF16),
        ed_v=vmem(expert_down.shape[1:], BF16),
        dd_v=vmem(dense_down.shape, BF16),
        send1=vmem((n * slot1, LANES), F32),
        recv1=vmem((n * slot1, LANES), F32),
        own_rows=vmem((16, width), F32),
        pack2=vmem((n * slot2, LANES), F32),
        send2=vmem((n * slot2, LANES), BF16),
        recv2=vmem((n * slot2, LANES), BF16),
        sum2=vmem((slot2, LANES), F32),
        small=vmem((small_rows, heads), F32),
        reads=vmem((8, gs), F32),
        old_read=vmem((8, half), F32),
        pack3=vmem((slot3, LANES), F32),
        send3=vmem((slot3, LANES), BF16),
        recv3=vmem((n * slot3, LANES), BF16),
        wide3=vmem((n * slot3, LANES), F32),
        turn=vmem((8, half), F32),
        send4=vmem((rows, LANES), F32),
        recv4=vmem((rows, LANES), F32),
        send5=vmem((rows, LANES), BF16),
        recv5=vmem((n * rows, LANES), BF16),
        hidden=vmem((rows, width), F32),
        pack6=vmem((rows * slot6, LANES), F32),
        send6=vmem((rows * slot6, LANES), BF16),
        recv6=vmem((n * nc * slot6, LANES), BF16),
        sum6=vmem((slot6, LANES), F32),
        load_sem=pltpu.SemaphoreType.DMA((13,)),
        send_sem=pltpu.SemaphoreType.DMA((6,)),
        recv_sem=pltpu.SemaphoreType.DMA((6,)),
    )
    in_vmem = pl.BlockSpec(memory_space=pltpu.VMEM)
    anywhere = pl.BlockSpec(memory_space=pl.ANY)
    names = tuple(small_in) + tuple(big_in) + tuple(outs)
    layer_out, state_out, inner_out, proj_out = pl.pallas_call(
        functools.partial(layer_kernel, n, nc, names, tuple(scratch)),
        out_shape=tuple(outs.values()),
        in_specs=[in_vmem] * len(small_in) + [anywhere] * len(big_in),
        out_specs=(in_vmem, anywhere, in_vmem, in_vmem),
        scratch_shapes=list(scratch.values()),
        compiler_params=pltpu.CompilerParams(
            collective_id=0, has_side_effects=True, vmem_limit_bytes=60 * 1024 * 1024
        ),
    )(*small_in.values(), *big_in.values())
    conv_out = jnp.concatenate([conv_state[:, 1:], inner_out[:, None]], axis=1)
    conv_proj_out = jnp.concatenate(
        [conv_proj_state[:, 1:], proj_out.reshape(q, 1, 2, gs)], axis=1
    )
    return (layer_out, state_out.reshape(head_state.shape), conv_out, conv_proj_out)


def solution(mesh):
    n, nc = mesh.shape["ep"], mesh.shape["tp"]
    placed = (
        P("ep", None),
        P("ep", "tp", None, None),
        P("ep", None, "tp"),
        P("ep", None, None, "tp"),
        P(),
        P("ep", "tp"),
        P("ep", "tp"),
        P(None, "tp"),
        P(None, "tp"),
        P(None, "tp"),
        P(None, "tp"),
        P(None, None, "tp"),
        P("tp"),
        P("tp"),
        P("tp"),
        P("tp"),
        P("tp", "ep"),
        P(),
        P("ep", None),
        P("ep", None),
        P("ep", None, "tp"),
        P("ep", None, "tp"),
        P("ep", "tp", None),
        P(None, ("ep", "tp")),
        P(("ep", "tp"), None),
        P(),
    )

    def body(*args):
        seq, width = args[0].shape
        if width == n * LANES and seq == nc and args[5].shape[1] % LANES == 0:
            return fused_local(n, nc, *args)
        return local(*args)

    return jax.shard_map(
        body,
        mesh=mesh,
        in_specs=placed,
        out_specs=(
            P(("ep", "tp"), None),
            P("ep", "tp", None, None),
            P("ep", None, "tp"),
            P("ep", None, None, "tp"),
        ),
        check_vma=False,
    )
```

```python
import functools
import types

import jax
import jax.numpy as jnp
from jax import lax
from jax.experimental import pallas as pl
from jax.experimental.pallas import tpu as pltpu
from jax.sharding import PartitionSpec as P

GROUPS = 4


norm_eps = 1e-05
clamp_limit = 7.0
glu_alpha = 1.702
highest = lax.Precision.HIGHEST


def rms_scale(values, gain_vec):
    return (
        values * lax.rsqrt(jnp.mean(values * values, axis=-1, keepdims=True) + norm_eps) * gain_vec
    )


def clamped_unit(gate_pre, up_pre):
    glu_part = jnp.minimum(gate_pre, clamp_limit)
    lin_part = jnp.clip(up_pre, -clamp_limit, clamp_limit)
    return glu_part * jax.nn.sigmoid(glu_alpha * glu_part) * (lin_part + 1.0)


def state_step(
    inner_proj,
    gate_proj,
    write_proj,
    read_proj,
    step_raw,
    conv_state,
    conv_proj_state,
    conv_kernel,
    conv_proj_kernel,
    step_bias,
    log_rate,
    skip_gain,
    group_gain,
    head_state,
    group_count,
):
    window_inner = jnp.concatenate([conv_state, inner_proj[:, None, :]], axis=1)
    window_proj = jnp.concatenate(
        [conv_proj_state, jnp.stack([write_proj, read_proj], axis=1)[:, None]], axis=1
    )
    conv_inner = jax.nn.silu(jnp.sum(window_inner.astype(jnp.float32) * conv_kernel[None], axis=1))
    conv_proj = jax.nn.silu(
        jnp.sum(window_proj.astype(jnp.float32) * conv_proj_kernel[None], axis=1)
    )
    seq_count, channels = conv_inner.shape
    head_count = step_raw.shape[1]
    head_width = channels // head_count
    state_width = conv_proj.shape[2] // group_count
    per_group = head_count // group_count
    head_input = conv_inner.reshape(seq_count, head_count, head_width)
    write_heads = jnp.repeat(
        conv_proj[:, 0].reshape(seq_count, group_count, state_width), per_group, axis=1
    )
    read_heads = jnp.repeat(
        conv_proj[:, 1].reshape(seq_count, group_count, state_width), per_group, axis=1
    )
    step_size = jax.nn.softplus(step_raw + step_bias)
    decay_rate = jnp.exp(-jnp.exp(log_rate) * step_size)
    state_out = (
        decay_rate[:, :, None, None] * head_state
        + (step_size[:, :, None] * head_input)[:, :, :, None] * write_heads[:, :, None, :]
    )
    read_out = (
        jnp.einsum("shpn,shn->shp", state_out, read_heads, precision=highest)
        + skip_gain[None, :, None] * head_input
    )
    gated_rows = read_out.reshape(seq_count, channels) * jax.nn.silu(gate_proj.astype(jnp.float32))
    grouped = gated_rows.reshape(seq_count, group_count, channels // group_count)
    grouped = grouped * lax.rsqrt(jnp.mean(grouped * grouped, axis=-1, keepdims=True) + norm_eps)
    mixer_rows = (grouped.reshape(seq_count, channels) * group_gain).astype(jnp.bfloat16)
    return (mixer_rows, state_out, window_inner[:, 1:], window_proj[:, 1:])


def local(
    tokens,
    head_state,
    conv_state,
    conv_proj_state,
    first_gain,
    gate_weight,
    inner_weight,
    write_weight,
    read_weight,
    step_weight,
    conv_kernel,
    conv_proj_kernel,
    step_bias,
    log_rate,
    skip_gain,
    group_gain,
    out_weight,
    second_gain,
    routes,
    route_logits,
    expert_gate,
    expert_up,
    expert_down,
    dense_up,
    dense_down,
    dense_gate,
):
    seq_count = tokens.shape[0]
    half_width = gate_weight.shape[1]
    normed_in = rms_scale(tokens.astype(jnp.float32), first_gain).astype(jnp.bfloat16)
    features = lax.all_to_all(normed_in, "ep", split_axis=1, concat_axis=0, tiled=True)
    row_block = features
    both_terms = lax.psum_scatter(
        jnp.concatenate(
            [
                jnp.dot(row_block, gate_weight, preferred_element_type=jnp.float32),
                jnp.dot(row_block, inner_weight, preferred_element_type=jnp.float32),
            ],
            axis=1,
        ),
        "ep",
        scatter_dimension=0,
        tiled=True,
    )
    gate_sum = both_terms[:, :half_width]
    inner_sum = both_terms[:, half_width:]
    gate_proj = gate_sum.astype(jnp.bfloat16)
    inner_proj = inner_sum.astype(jnp.bfloat16)
    write_proj = jnp.dot(normed_in, write_weight, preferred_element_type=jnp.float32).astype(
        jnp.bfloat16
    )
    read_proj = jnp.dot(normed_in, read_weight, preferred_element_type=jnp.float32).astype(
        jnp.bfloat16
    )
    step_raw = jnp.dot(normed_in, step_weight, preferred_element_type=jnp.float32)
    local_groups = GROUPS // lax.axis_size("tp")
    mixer_rows, state_out, conv_out, conv_proj_out = state_step(
        inner_proj,
        gate_proj,
        write_proj,
        read_proj,
        step_raw,
        conv_state,
        conv_proj_state,
        conv_kernel,
        conv_proj_kernel,
        step_bias,
        log_rate,
        skip_gain,
        group_gain,
        head_state,
        local_groups,
    )
    partial_mix = jnp.dot(
        mixer_rows,
        lax.all_gather(out_weight, "ep", axis=1, tiled=True),
        preferred_element_type=jnp.float32,
    )
    mixed = lax.psum(partial_mix, "tp")
    hidden = (tokens.astype(jnp.float32) + mixed).astype(jnp.bfloat16)
    normed_mid = rms_scale(hidden.astype(jnp.float32), second_gain).astype(jnp.bfloat16)
    all_rows, all_routes, all_logits = (
        lax.all_gather(normed_mid, "ep", axis=0, tiled=True),
        lax.all_gather(routes, "ep", axis=0, tiled=True),
        lax.all_gather(route_logits, "ep", axis=0, tiled=True),
    )
    route_gates = jax.nn.softmax(all_logits.astype(jnp.float32), axis=-1)
    my_expert = lax.axis_index("ep")
    route_hits = all_routes == my_expert
    row_weight = jnp.sum(jnp.where(route_hits, route_gates, 0.0), axis=1)
    chosen = jnp.any(route_hits, axis=1)
    slot_index = jnp.cumsum(chosen.astype(jnp.int32)) - 1
    capacity = 4 * seq_count * routes.shape[1]
    slot_ids = jnp.arange(capacity, dtype=jnp.int32)
    picks = (slot_index[None, :] == slot_ids[:, None]) & chosen[None, :]
    picked_rows = jnp.dot(
        picks.astype(jnp.bfloat16), all_rows, preferred_element_type=jnp.float32
    ).astype(jnp.bfloat16)
    activated = clamped_unit(
        jnp.dot(picked_rows, expert_gate[0], preferred_element_type=jnp.float32),
        jnp.dot(picked_rows, expert_up[0], preferred_element_type=jnp.float32),
    ).astype(jnp.bfloat16)
    expert_part = jnp.dot(activated, expert_down[0], preferred_element_type=jnp.float32)
    placed = jnp.where(picks, row_weight[None, :], 0.0)
    dense_weight = jax.nn.sigmoid(
        jnp.dot(all_rows.astype(jnp.float32), dense_gate, precision=highest)
    )
    row_share = seq_count // lax.axis_size("tp")
    row_block = all_rows
    dense_inner = jax.nn.silu(
        jnp.dot(row_block, dense_up, preferred_element_type=jnp.float32)
    ).astype(jnp.bfloat16)
    dense_term = (
        jnp.dot(dense_inner, dense_down, preferred_element_type=jnp.float32) * dense_weight[:, None]
    )
    summed = lax.psum_scatter(
        dense_term + jnp.einsum("cr,cd->rd", placed, expert_part, precision=highest),
        ("ep", "tp"),
        scatter_dimension=0,
        tiled=True,
    )
    own_rows = lax.dynamic_slice_in_dim(hidden, lax.axis_index("tp") * row_share, row_share, 0)
    layer_out = (own_rows.astype(jnp.float32) + summed).astype(jnp.bfloat16)
    return (layer_out, state_out, conv_out, conv_proj_out)


LANES = 128
MESH = pl.DeviceIdType.MESH
F32 = jnp.float32
BF16 = jnp.bfloat16


def silu(x):
    return x * jax.nn.sigmoid(x)


def dot(a, b):
    return jnp.dot(a, b, preferred_element_type=F32)


def lanes_of(ref, start, count, stride, pieces):
    return jnp.concatenate(
        [ref[pl.ds(start + j, count, stride=stride), :] for j in range(pieces)], axis=1
    )


def layer_kernel(
    n,
    nc,
    names,
    scratch_names,
    *refs,
):
    r = types.SimpleNamespace(**dict(zip(names + scratch_names, refs)))
    me = lax.axis_index("ep")
    core = lax.axis_index("tp")
    q = r.tokens.shape[0]
    width = r.tokens.shape[1]
    half = r.gate_v.shape[1]
    chunks = half // LANES
    wide_chunks = width // LANES
    rows = n * q
    slot1 = r.send1.shape[0] // n
    slot2 = 2 * q * chunks
    slot3 = q * chunks
    slot6 = wide_chunks
    heads = r.step_bias.shape[1]
    head_width = half // heads
    state_width = r.hs.shape[2]
    groups = r.write_v.shape[1] // state_width
    group_width = half // groups
    topk = r.routes.shape[1]

    barrier = pltpu.get_barrier_semaphore()

    def greet(step, _):
        other = lax.rem(me * nc + core + step, n * nc)
        pl.semaphore_signal(
            barrier, inc=1, device_id=(other // nc, lax.rem(other, nc)), device_id_type=MESH
        )
        return 0

    lax.fori_loop(1, n * nc, greet, 0)

    order = (
        (r.gate_weight, r.gate_v),
        (r.inner_weight, r.inner_v),
        (r.write_weight, r.write_v),
        (r.read_weight, r.read_v),
        (r.step_weight, r.step_v),
        (r.head_state, r.hs),
        (r.out_weight, r.out_v),
        (r.expert_gate, r.eg_v),
        (r.expert_up, r.eu_v),
        (r.dense_up, r.du_v),
        (r.expert_down, r.ed_v),
        (r.dense_down, r.dd_v),
    )
    loads = [
        pltpu.make_async_copy(src, dst, r.load_sem.at[i]) for i, (src, dst) in enumerate(order)
    ]
    for load in loads:
        load.start()
    (
        gate_load,
        inner_load,
        write_load,
        read_load,
        step_load,
        state_load,
        out_load,
        expert_gate_load,
        expert_up_load,
        dense_up_load,
        expert_down_load,
        dense_down_load,
    ) = loads

    def all_to_all(phase, send, recv, slot, same=False):
        def one(step, _):
            peer = lax.rem(me + step, n)
            src = send if same else send.at[pl.ds(pl.multiple_of(peer * slot, slot), slot)]
            pltpu.make_async_remote_copy(
                src_ref=src,
                dst_ref=recv.at[pl.ds(pl.multiple_of(me * slot, slot), slot)],
                send_sem=r.send_sem.at[phase],
                recv_sem=r.recv_sem.at[phase],
                device_id=(peer, core),
                device_id_type=MESH,
            ).start()
            return 0

        lax.fori_loop(1, n, one, 0)

    def drain(sem, buffer, count):
        part = buffer.at[pl.ds(0, count)]
        pltpu.make_async_copy(part, part, sem).wait()

    def take(phase, send, recv, slot, same=False):
        drain(r.recv_sem.at[phase], recv, (n - 1) * slot)
        mine = pl.ds(pl.multiple_of(me * slot, slot), slot)
        recv[mine, :] = send[...] if same else send[mine, :]

    x = r.tokens[...].astype(F32)
    normed = rms_scale(x, r.first_gain[...]).astype(BF16).astype(F32)
    send1 = r.send1
    send1[...] = jnp.zeros_like(send1)
    chosen = r.routes[...].astype(F32)
    scores = r.route_logits[...].astype(F32)
    for e in range(n):
        at, cut = e * slot1, slice(e * LANES, (e + 1) * LANES)
        send1[at : at + q, :] = normed[:, cut]
        send1[at + q : at + 2 * q, :] = x[:, cut]
        send1[at + 2 * q : at + 3 * q, 0:topk] = chosen
        send1[at + 3 * q : at + 4 * q, 0:topk] = scores
    pl.semaphore_wait(barrier, n * nc - 1)
    all_to_all(0, send1, r.recv1, slot1)

    own = r.own_rows
    own[...] = jnp.zeros_like(own)
    own[0:q, :] = normed
    own_b = own[...].astype(BF16)
    gate_load.wait()
    inner_load.wait()
    write_load.wait()
    read_load.wait()
    step_load.wait()
    write_proj = dot(own_b, r.write_v[...])[0:q].astype(BF16)
    read_proj = dot(own_b, r.read_v[...])[0:q].astype(BF16)
    step_raw = lax.dot_general(
        own_b, r.step_v[...], (((1,), (1,)), ((), ())), preferred_element_type=F32
    )[0:q]

    take(0, send1, r.recv1, slot1)
    recv1 = r.recv1

    def gathered(offset):
        return jnp.concatenate(
            [recv1[pl.ds(offset + s, n, stride=slot1), :] for s in range(q)], axis=0
        )

    features = gathered(0).astype(BF16)
    pack2 = r.pack2
    for g, weight in enumerate((r.gate_v, r.inner_v)):
        part = dot(features, weight[...])
        for s in range(q):
            for j in range(chunks):
                pack2[pl.ds((s * 2 + g) * chunks + j, n, stride=slot2), :] = part[
                    s * n : (s + 1) * n, j * LANES : (j + 1) * LANES
                ]
    r.send2[...] = pack2[...].astype(BF16)
    all_to_all(1, r.send2, r.recv2, slot2)

    gs = groups * state_width
    taps = r.conv_kernel.shape[0]
    for s in range(q):
        fresh = r.fresh
        fresh[0:1, :] = write_proj[s : s + 1].astype(F32)
        fresh[1:2, :] = read_proj[s : s + 1].astype(F32)
        newest = fresh[0:2, :]
        r.proj_out[s, taps - 2] = newest.astype(BF16)
        window = newest * r.conv_proj_kernel[taps - 1]
        for j in range(taps - 1):
            held = r.conv_proj_state[s, j]
            if j > 0:
                r.proj_out[s, j - 1] = held
            window += held.astype(F32) * r.conv_proj_kernel[j]
        window = silu(window)
        r.vectors[s : s + 1, 0:gs] = window[0:1]
        r.vectors[s : s + 1, gs:] = window[1:2]
    write, read = r.vectors[0:q, 0:gs], r.vectors[0:q, gs:]
    inner_part = jnp.zeros((q, half), F32)
    for j in range(taps - 1):
        held = r.conv_state[j]
        if j > 0:
            r.conv_out[j - 1] = held
        inner_part += held.astype(F32) * r.conv_kernel[j : j + 1, :]
    pre = step_raw + r.step_bias[...]
    step_size = jnp.maximum(pre, 0.0) + jnp.log1p(jnp.exp(-jnp.abs(pre)))
    decay = jnp.exp(-jnp.exp(r.log_rate[...]) * step_size)
    small = r.small
    small[...] = jnp.zeros_like(small)
    small[0:q, :] = step_size
    small[q : 2 * q, :] = decay
    small[2 * q : 2 * q + 1, :] = r.skip_gain[...]
    spread = (
        lax.broadcasted_iota(jnp.int32, (heads, half), 1) // head_width
        == lax.broadcasted_iota(jnp.int32, (heads, half), 0)
    ).astype(F32)
    by_channel = jnp.dot(small[...], spread, precision=highest, preferred_element_type=F32)
    step_rows, decay_rows = by_channel[0:q], by_channel[q : 2 * q]
    skip_rows = by_channel[2 * q : 2 * q + 1]
    reads = r.reads
    reads[...] = jnp.zeros_like(reads)
    reads[0:q, :] = read
    state_load.wait()
    old_read = r.old_read
    write_read = []
    for g in range(groups):
        lane = slice(g * state_width, (g + 1) * state_width)
        span = slice(g * group_width, (g + 1) * group_width)
        write_read.append(
            jnp.broadcast_to(
                jnp.sum(write[:, lane] * read[:, lane], axis=1, keepdims=True), (q, group_width)
            )
        )
        for s in range(q):
            old_read[s : s + 1, span] = lax.dot_general(
                reads[:, lane],
                r.hs[s, span, :],
                (((1,), (1,)), ((), ())),
                precision=highest,
                preferred_element_type=F32,
            )[s : s + 1]
    carried = decay_rows * old_read[0:q, :]
    direct = step_rows * jnp.concatenate(write_read, axis=1) + skip_rows

    all_routes, all_scores = gathered(2 * q), gathered(3 * q)
    real = lax.broadcasted_iota(jnp.int32, (rows, LANES), 1) < topk
    top = jnp.max(jnp.where(real, all_scores, -jnp.inf), axis=1, keepdims=True)
    raised = jnp.where(real, jnp.exp(jnp.where(real, all_scores - top, 0.0)), 0.0)
    gates = raised / jnp.sum(raised, axis=1, keepdims=True)
    hits = real & (all_routes == me.astype(F32))
    row_weight = jnp.sum(jnp.where(hits, gates, 0.0), axis=1, keepdims=True)

    take(1, r.send2, r.recv2, slot2)
    total = r.recv2[0:slot2, :].astype(F32)
    for e in range(1, n):
        total += r.recv2[e * slot2 : (e + 1) * slot2, :].astype(F32)
    r.sum2[...] = total
    gate_proj = lanes_of(r.sum2, 0, q, 2 * chunks, chunks).astype(BF16).astype(F32)
    inner_proj = lanes_of(r.sum2, chunks, q, 2 * chunks, chunks).astype(BF16)
    conv_inner = silu(inner_part + inner_proj.astype(F32) * r.conv_kernel[taps - 1 : taps, :])
    gated = (carried + direct * conv_inner) * silu(gate_proj)
    normal = []
    for g in range(groups):
        piece = gated[:, g * group_width : (g + 1) * group_width]
        normal.append(
            piece * lax.rsqrt(jnp.mean(piece * piece, axis=1, keepdims=True) + norm_eps)
        )
    mixer = jnp.concatenate(normal, axis=1) * r.group_gain[...]
    for j in range(chunks):
        r.pack3[pl.ds(j, q, stride=chunks), :] = mixer[:, j * LANES : (j + 1) * LANES]
    r.send3[...] = r.pack3[...].astype(BF16)
    all_to_all(2, r.send3, r.recv3, slot3, same=True)

    r.conv_out[taps - 2] = inner_proj
    turn = r.turn
    turn[...] = jnp.zeros_like(turn)
    turn[0:q, :] = decay_rows
    turn[q : 2 * q, :] = step_rows * conv_inner
    columns = jnp.transpose(turn[...])
    for s in range(q):
        for k in range(chunks):
            span = slice(k * LANES, (k + 1) * LANES)
            g = k * LANES // group_width
            r.state_out[s, span, :] = (
                columns[span, s : s + 1] * r.hs[s, span, :]
                + columns[span, q + s : q + s + 1]
                * write[s : s + 1, g * state_width : (g + 1) * state_width]
            )
    raw_block = gathered(q)
    out_load.wait()

    take(2, r.send3, r.recv3, slot3, same=True)
    r.wide3[...] = r.recv3[...].astype(F32)
    all_mixer = jnp.concatenate(
        [lanes_of(r.wide3, s * chunks, n, slot3, chunks) for s in range(q)], axis=0
    ).astype(BF16)
    part = dot(all_mixer, r.out_v[...])
    r.send4[...] = part
    swap = pltpu.make_async_remote_copy(
        src_ref=r.send4,
        dst_ref=r.recv4,
        send_sem=r.send_sem.at[3],
        recv_sem=r.recv_sem.at[3],
        device_id=(me, lax.rem(core + 1, nc)),
        device_id_type=MESH,
    )
    swap.start()
    swap.wait_recv()
    r.send5[...] = (raw_block + (part + r.recv4[...])).astype(BF16)
    all_to_all(4, r.send5, r.recv5, rows, same=True)
    expert_gate_load.wait()
    expert_up_load.wait()
    dense_up_load.wait()
    take(4, r.send5, r.recv5, rows, same=True)
    hidden = jnp.concatenate(
        [r.recv5[e * rows : (e + 1) * rows, :] for e in range(n)], axis=1
    ).astype(F32)
    r.hidden[...] = hidden
    mid = rms_scale(hidden, r.second_gain[...]).astype(BF16)
    dense_inner = silu(dot(mid, r.du_v[...])).astype(BF16)
    activated = clamped_unit(dot(mid, r.eg_v[...]), dot(mid, r.eu_v[...])).astype(BF16)
    dense_weight = jax.nn.sigmoid(
        jnp.sum(mid.astype(F32) * r.dense_gate[...], axis=1, keepdims=True)
    )
    expert_down_load.wait()
    dense_down_load.wait()
    cuts = 4
    for c in range(cuts):
        span = slice(c * width // cuts, (c + 1) * width // cuts)
        term = dot(activated, r.ed_v[:, span]) * row_weight
        term += dot(dense_inner, r.dd_v[:, span]) * dense_weight
        for j in range(wide_chunks // cuts):
            r.pack6[pl.ds(c * wide_chunks // cuts + j, rows, stride=slot6), :] = term[
                :, j * LANES : (j + 1) * LANES
            ]
    r.send6[...] = r.pack6[...].astype(BF16)
    mine = me * nc + core

    def one(step, _):
        other = lax.rem(mine + step, n * nc)
        peer, peer_core = other // nc, lax.rem(other, nc)
        pltpu.make_async_remote_copy(
            src_ref=r.send6.at[
                pl.ds(pl.multiple_of((peer_core * n + peer) * slot6, slot6), slot6)
            ],
            dst_ref=r.recv6.at[pl.ds(pl.multiple_of(mine * slot6, slot6), slot6)],
            send_sem=r.send_sem.at[5],
            recv_sem=r.recv_sem.at[5],
            device_id=(peer, peer_core),
            device_id_type=MESH,
        ).start()
        return 0

    lax.fori_loop(1, n * nc, one, 0)
    own_row = r.hidden[pl.ds(core * n + me, 1), :]
    drain(r.recv_sem.at[5], r.recv6, (n * nc - 1) * slot6)
    r.recv6[pl.ds(pl.multiple_of(mine * slot6, slot6), slot6), :] = r.send6[
        pl.ds(pl.multiple_of((core * n + me) * slot6, slot6), slot6), :
    ]
    total = r.recv6[0:slot6, :].astype(F32)
    for e in range(1, n * nc):
        total += r.recv6[e * slot6 : (e + 1) * slot6, :].astype(F32)
    r.sum6[...] = total
    summed = jnp.concatenate([r.sum6[j : j + 1, :] for j in range(wide_chunks)], axis=1)
    r.layer_out[...] = (own_row + summed).astype(BF16)

    drain(r.send_sem.at[0], send1, (n - 1) * slot1)
    drain(r.send_sem.at[1], r.send2, (n - 1) * slot2)
    drain(r.send_sem.at[2], r.recv3, (n - 1) * slot3)
    swap.wait_send()
    drain(r.send_sem.at[4], r.recv5, (n - 1) * rows)
    drain(r.send_sem.at[5], r.send6, (n * nc - 1) * slot6)


def store_kernel(*refs):
    count = len(refs) // 2
    copies = [
        pltpu.make_async_copy(refs[i], refs[count + i], refs[-1].at[i]) for i in range(count)
    ]
    for copy in copies:
        copy.start()
    for copy in copies:
        copy.wait()


def fused_local(
    n,
    nc,
    tokens,
    head_state,
    conv_state,
    conv_proj_state,
    first_gain,
    gate_weight,
    inner_weight,
    write_weight,
    read_weight,
    step_weight,
    conv_kernel,
    conv_proj_kernel,
    step_bias,
    log_rate,
    skip_gain,
    group_gain,
    out_weight,
    second_gain,
    routes,
    route_logits,
    expert_gate,
    expert_up,
    expert_down,
    dense_up,
    dense_down,
    dense_gate,
):
    q, width = tokens.shape
    half = gate_weight.shape[1]
    rows = n * q
    chunks, wide_chunks = half // LANES, width // LANES
    gs = write_weight.shape[1]
    heads, state_width = head_state.shape[1], head_state.shape[3]
    taps = conv_kernel.shape[0]
    small_in = dict(
        tokens=tokens,
        first_gain=first_gain[None],
        conv_state=jnp.transpose(conv_state, (1, 0, 2)),
        conv_proj_state=conv_proj_state,
        conv_kernel=conv_kernel,
        conv_proj_kernel=conv_proj_kernel,
        step_bias=step_bias[None],
        log_rate=log_rate[None],
        skip_gain=skip_gain[None],
        group_gain=group_gain[None],
        second_gain=second_gain[None],
        routes=routes,
        route_logits=route_logits,
        dense_gate=dense_gate[None],
    )
    big_in = dict(
        head_state=head_state.reshape(q, half, state_width),
        gate_weight=gate_weight,
        inner_weight=inner_weight,
        write_weight=write_weight,
        read_weight=read_weight,
        step_weight=step_weight.T,
        out_weight=out_weight,
        expert_gate=expert_gate[0],
        expert_up=expert_up[0],
        expert_down=expert_down[0],
        dense_up=dense_up,
        dense_down=dense_down,
    )
    vmem = pltpu.VMEM
    outs = dict(
        layer_out=vmem((q // nc, width), BF16),
        state_out=vmem((q, half, state_width), F32),
        conv_out=vmem((taps - 1, q, half), BF16),
        proj_out=vmem((q, taps - 1, 2, gs), BF16),
    )
    slot1 = -(-4 * q // 8) * 8
    slot2, slot3, slot6 = 2 * q * chunks, q * chunks, wide_chunks
    small_rows = -(-(2 * q + 1) // 8) * 8
    scratch = dict(
        gate_v=vmem(gate_weight.shape, BF16),
        inner_v=vmem(inner_weight.shape, BF16),
        write_v=vmem(write_weight.shape, BF16),
        read_v=vmem(read_weight.shape, BF16),
        step_v=vmem(step_weight.shape[::-1], BF16),
        hs=vmem((q, half, state_width), F32),
        out_v=vmem(out_weight.shape, BF16),
        eg_v=vmem(expert_gate.shape[1:], BF16),
        eu_v=vmem(expert_up.shape[1:], BF16),
        du_v=vmem(dense_up.shape, BF16),
        ed_v=vmem(expert_down.shape[1:], BF16),
        dd_v=vmem(dense_down.shape, BF16),
        send1=vmem((n * slot1, LANES), F32),
        recv1=vmem((n * slot1, LANES), F32),
        own_rows=vmem((16, width), F32),
        pack2=vmem((n * slot2, LANES), F32),
        send2=vmem((n * slot2, LANES), BF16),
        recv2=vmem((n * slot2, LANES), BF16),
        sum2=vmem((slot2, LANES), F32),
        fresh=vmem((8, gs), F32),
        vectors=vmem((8, 2 * gs), F32),
        small=vmem((small_rows, heads), F32),
        reads=vmem((8, gs), F32),
        old_read=vmem((8, half), F32),
        pack3=vmem((slot3, LANES), F32),
        send3=vmem((slot3, LANES), BF16),
        recv3=vmem((n * slot3, LANES), BF16),
        wide3=vmem((n * slot3, LANES), F32),
        turn=vmem((8, half), F32),
        send4=vmem((rows, LANES), F32),
        recv4=vmem((rows, LANES), F32),
        send5=vmem((rows, LANES), BF16),
        recv5=vmem((n * rows, LANES), BF16),
        hidden=vmem((rows, width), F32),
        pack6=vmem((rows * slot6, LANES), F32),
        send6=vmem((rows * slot6, LANES), BF16),
        recv6=vmem((n * nc * slot6, LANES), BF16),
        sum6=vmem((slot6, LANES), F32),
        load_sem=pltpu.SemaphoreType.DMA((12,)),
        send_sem=pltpu.SemaphoreType.DMA((6,)),
        recv_sem=pltpu.SemaphoreType.DMA((6,)),
    )
    in_vmem = pl.BlockSpec(memory_space=pltpu.VMEM)
    anywhere = pl.BlockSpec(memory_space=pl.ANY)
    names = tuple(small_in) + tuple(big_in) + tuple(outs)
    results = pl.pallas_call(
        functools.partial(layer_kernel, n, nc, names, tuple(scratch)),
        out_shape=tuple(outs.values()),
        in_specs=[in_vmem] * len(small_in) + [anywhere] * len(big_in),
        out_specs=(in_vmem,) * len(outs),
        scratch_shapes=list(scratch.values()),
        compiler_params=pltpu.CompilerParams(
            collective_id=0, has_side_effects=True, vmem_limit_bytes=60 * 1024 * 1024
        ),
    )(*small_in.values(), *big_in.values())
    layer_out, state_out, conv_out, proj_out = pl.pallas_call(
        store_kernel,
        out_shape=tuple(jax.ShapeDtypeStruct(a.shape, a.dtype) for a in results),
        in_specs=[in_vmem] * len(results),
        out_specs=(anywhere,) * len(results),
        scratch_shapes=[pltpu.SemaphoreType.DMA((len(results),))],
    )(*[pltpu.with_memory_space_constraint(a, pltpu.VMEM) for a in results])
    return (
        layer_out,
        state_out.reshape(head_state.shape),
        jnp.transpose(conv_out, (1, 0, 2)),
        proj_out,
    )


def solution(mesh):
    n, nc = mesh.shape["ep"], mesh.shape["tp"]
    placed = (
        P("ep", None),
        P("ep", "tp", None, None),
        P("ep", None, "tp"),
        P("ep", None, None, "tp"),
        P(),
        P("ep", "tp"),
        P("ep", "tp"),
        P(None, "tp"),
        P(None, "tp"),
        P(None, "tp"),
        P(None, "tp"),
        P(None, None, "tp"),
        P("tp"),
        P("tp"),
        P("tp"),
        P("tp"),
        P("tp", "ep"),
        P(),
        P("ep", None),
        P("ep", None),
        P("ep", None, "tp"),
        P("ep", None, "tp"),
        P("ep", "tp", None),
        P(None, ("ep", "tp")),
        P(("ep", "tp"), None),
        P(),
    )

    def body(*args):
        seq, width = args[0].shape
        if width == n * LANES and seq == nc and args[5].shape[1] % LANES == 0:
            return fused_local(n, nc, *args)
        return local(*args)

    return jax.shard_map(
        body,
        mesh=mesh,
        in_specs=placed,
        out_specs=(
            P(("ep", "tp"), None),
            P("ep", "tp", None, None),
            P("ep", None, "tp"),
            P("ep", None, None, "tp"),
        ),
        check_vma=False,
    )
```

```python
import functools
import types

import jax
import jax.numpy as jnp
from jax import lax
from jax.experimental import pallas as pl
from jax.experimental.pallas import tpu as pltpu
from jax.sharding import PartitionSpec as P

GROUPS = 4


norm_eps = 1e-05
clamp_limit = 7.0
glu_alpha = 1.702
highest = lax.Precision.HIGHEST


def rms_scale(values, gain_vec):
    return (
        values * lax.rsqrt(jnp.mean(values * values, axis=-1, keepdims=True) + norm_eps) * gain_vec
    )


def clamped_unit(gate_pre, up_pre):
    glu_part = jnp.minimum(gate_pre, clamp_limit)
    lin_part = jnp.clip(up_pre, -clamp_limit, clamp_limit)
    return glu_part * jax.nn.sigmoid(glu_alpha * glu_part) * (lin_part + 1.0)


def state_step(
    inner_proj,
    gate_proj,
    write_proj,
    read_proj,
    step_raw,
    conv_state,
    conv_proj_state,
    conv_kernel,
    conv_proj_kernel,
    step_bias,
    log_rate,
    skip_gain,
    group_gain,
    head_state,
    group_count,
):
    window_inner = jnp.concatenate([conv_state, inner_proj[:, None, :]], axis=1)
    window_proj = jnp.concatenate(
        [conv_proj_state, jnp.stack([write_proj, read_proj], axis=1)[:, None]], axis=1
    )
    conv_inner = jax.nn.silu(jnp.sum(window_inner.astype(jnp.float32) * conv_kernel[None], axis=1))
    conv_proj = jax.nn.silu(
        jnp.sum(window_proj.astype(jnp.float32) * conv_proj_kernel[None], axis=1)
    )
    seq_count, channels = conv_inner.shape
    head_count = step_raw.shape[1]
    head_width = channels // head_count
    state_width = conv_proj.shape[2] // group_count
    per_group = head_count // group_count
    head_input = conv_inner.reshape(seq_count, head_count, head_width)
    write_heads = jnp.repeat(
        conv_proj[:, 0].reshape(seq_count, group_count, state_width), per_group, axis=1
    )
    read_heads = jnp.repeat(
        conv_proj[:, 1].reshape(seq_count, group_count, state_width), per_group, axis=1
    )
    step_size = jax.nn.softplus(step_raw + step_bias)
    decay_rate = jnp.exp(-jnp.exp(log_rate) * step_size)
    state_out = (
        decay_rate[:, :, None, None] * head_state
        + (step_size[:, :, None] * head_input)[:, :, :, None] * write_heads[:, :, None, :]
    )
    read_out = (
        jnp.einsum("shpn,shn->shp", state_out, read_heads, precision=highest)
        + skip_gain[None, :, None] * head_input
    )
    gated_rows = read_out.reshape(seq_count, channels) * jax.nn.silu(gate_proj.astype(jnp.float32))
    grouped = gated_rows.reshape(seq_count, group_count, channels // group_count)
    grouped = grouped * lax.rsqrt(jnp.mean(grouped * grouped, axis=-1, keepdims=True) + norm_eps)
    mixer_rows = (grouped.reshape(seq_count, channels) * group_gain).astype(jnp.bfloat16)
    return (mixer_rows, state_out, window_inner[:, 1:], window_proj[:, 1:])


def local(
    tokens,
    head_state,
    conv_state,
    conv_proj_state,
    first_gain,
    gate_weight,
    inner_weight,
    write_weight,
    read_weight,
    step_weight,
    conv_kernel,
    conv_proj_kernel,
    step_bias,
    log_rate,
    skip_gain,
    group_gain,
    out_weight,
    second_gain,
    routes,
    route_logits,
    expert_gate,
    expert_up,
    expert_down,
    dense_up,
    dense_down,
    dense_gate,
):
    seq_count = tokens.shape[0]
    half_width = gate_weight.shape[1]
    normed_in = rms_scale(tokens.astype(jnp.float32), first_gain).astype(jnp.bfloat16)
    features = lax.all_to_all(normed_in, "ep", split_axis=1, concat_axis=0, tiled=True)
    row_block = features
    both_terms = lax.psum_scatter(
        jnp.concatenate(
            [
                jnp.dot(row_block, gate_weight, preferred_element_type=jnp.float32),
                jnp.dot(row_block, inner_weight, preferred_element_type=jnp.float32),
            ],
            axis=1,
        ),
        "ep",
        scatter_dimension=0,
        tiled=True,
    )
    gate_sum = both_terms[:, :half_width]
    inner_sum = both_terms[:, half_width:]
    gate_proj = gate_sum.astype(jnp.bfloat16)
    inner_proj = inner_sum.astype(jnp.bfloat16)
    write_proj = jnp.dot(normed_in, write_weight, preferred_element_type=jnp.float32).astype(
        jnp.bfloat16
    )
    read_proj = jnp.dot(normed_in, read_weight, preferred_element_type=jnp.float32).astype(
        jnp.bfloat16
    )
    step_raw = jnp.dot(normed_in, step_weight, preferred_element_type=jnp.float32)
    local_groups = GROUPS // lax.axis_size("tp")
    mixer_rows, state_out, conv_out, conv_proj_out = state_step(
        inner_proj,
        gate_proj,
        write_proj,
        read_proj,
        step_raw,
        conv_state,
        conv_proj_state,
        conv_kernel,
        conv_proj_kernel,
        step_bias,
        log_rate,
        skip_gain,
        group_gain,
        head_state,
        local_groups,
    )
    partial_mix = jnp.dot(
        mixer_rows,
        lax.all_gather(out_weight, "ep", axis=1, tiled=True),
        preferred_element_type=jnp.float32,
    )
    mixed = lax.psum(partial_mix, "tp")
    hidden = (tokens.astype(jnp.float32) + mixed).astype(jnp.bfloat16)
    normed_mid = rms_scale(hidden.astype(jnp.float32), second_gain).astype(jnp.bfloat16)
    all_rows, all_routes, all_logits = (
        lax.all_gather(normed_mid, "ep", axis=0, tiled=True),
        lax.all_gather(routes, "ep", axis=0, tiled=True),
        lax.all_gather(route_logits, "ep", axis=0, tiled=True),
    )
    route_gates = jax.nn.softmax(all_logits.astype(jnp.float32), axis=-1)
    my_expert = lax.axis_index("ep")
    route_hits = all_routes == my_expert
    row_weight = jnp.sum(jnp.where(route_hits, route_gates, 0.0), axis=1)
    chosen = jnp.any(route_hits, axis=1)
    slot_index = jnp.cumsum(chosen.astype(jnp.int32)) - 1
    capacity = 4 * seq_count * routes.shape[1]
    slot_ids = jnp.arange(capacity, dtype=jnp.int32)
    picks = (slot_index[None, :] == slot_ids[:, None]) & chosen[None, :]
    picked_rows = jnp.dot(
        picks.astype(jnp.bfloat16), all_rows, preferred_element_type=jnp.float32
    ).astype(jnp.bfloat16)
    activated = clamped_unit(
        jnp.dot(picked_rows, expert_gate[0], preferred_element_type=jnp.float32),
        jnp.dot(picked_rows, expert_up[0], preferred_element_type=jnp.float32),
    ).astype(jnp.bfloat16)
    expert_part = jnp.dot(activated, expert_down[0], preferred_element_type=jnp.float32)
    placed = jnp.where(picks, row_weight[None, :], 0.0)
    dense_weight = jax.nn.sigmoid(
        jnp.dot(all_rows.astype(jnp.float32), dense_gate, precision=highest)
    )
    row_share = seq_count // lax.axis_size("tp")
    row_block = all_rows
    dense_inner = jax.nn.silu(
        jnp.dot(row_block, dense_up, preferred_element_type=jnp.float32)
    ).astype(jnp.bfloat16)
    dense_term = (
        jnp.dot(dense_inner, dense_down, preferred_element_type=jnp.float32) * dense_weight[:, None]
    )
    summed = lax.psum_scatter(
        dense_term + jnp.einsum("cr,cd->rd", placed, expert_part, precision=highest),
        ("ep", "tp"),
        scatter_dimension=0,
        tiled=True,
    )
    own_rows = lax.dynamic_slice_in_dim(hidden, lax.axis_index("tp") * row_share, row_share, 0)
    layer_out = (own_rows.astype(jnp.float32) + summed).astype(jnp.bfloat16)
    return (layer_out, state_out, conv_out, conv_proj_out)


LANES = 128
MESH = pl.DeviceIdType.MESH
F32 = jnp.float32
BF16 = jnp.bfloat16


def silu(x):
    return x * jax.nn.sigmoid(x)


def dot(a, b):
    return jnp.dot(a, b, preferred_element_type=F32)


def lanes_of(ref, start, count, stride, pieces):
    return jnp.concatenate(
        [ref[pl.ds(start + j, count, stride=stride), :] for j in range(pieces)], axis=1
    )


def layer_kernel(
    n,
    nc,
    small_names,
    names,
    scratch_names,
    *refs,
):
    small_count = len(small_names)
    small_src, refs = refs[:small_count], refs[small_count:]
    r = types.SimpleNamespace(**dict(zip(names + scratch_names + small_names, refs)))
    small_dst = refs[len(refs) - small_count :]
    me = lax.axis_index("ep")
    core = lax.axis_index("tp")
    q, width = r.tokens.shape
    half = r.gate_v.shape[1]
    chunks = half // LANES
    wide_chunks = width // LANES
    rows = n * q
    slot0 = r.send0.shape[0] // n
    slot2 = 2 * q * chunks
    slot3 = q * chunks
    slot6 = wide_chunks
    heads = r.step_bias.shape[1]
    head_width = half // heads
    state_width = r.hs.shape[2]
    groups = r.write_v.shape[1] // state_width
    group_width = half // groups
    topk = r.routes.shape[1]

    barrier = pltpu.get_barrier_semaphore()

    def greet(step, _):
        other = lax.rem(me * nc + core + step, n * nc)
        pl.semaphore_signal(
            barrier, inc=1, device_id=(other // nc, lax.rem(other, nc)), device_id_type=MESH
        )
        return 0

    lax.fori_loop(1, n * nc, greet, 0)

    small_loads = [
        pltpu.make_async_copy(src, dst, r.small_sem.at[i])
        for i, (src, dst) in enumerate(zip(small_src, small_dst))
    ]
    for load in small_loads:
        load.start()
    order = (
        (r.gate_weight, r.gate_v),
        (r.inner_weight, r.inner_v),
        (r.write_weight, r.write_v),
        (r.read_weight, r.read_v),
        (r.step_weight, r.step_v),
        (r.head_state, r.hs),
        (r.out_weight, r.out_v),
        (r.expert_gate, r.eg_v),
        (r.expert_up, r.eu_v),
        (r.dense_up, r.du_v),
        (r.expert_down, r.ed_v),
        (r.dense_down, r.dd_v),
    )
    loads = [
        pltpu.make_async_copy(src, dst, r.load_sem.at[i]) for i, (src, dst) in enumerate(order)
    ]
    (
        gate_load,
        inner_load,
        write_load,
        read_load,
        step_load,
        state_load,
        out_load,
        expert_gate_load,
        expert_up_load,
        dense_up_load,
        expert_down_load,
        dense_down_load,
    ) = loads
    gate_load.start()
    inner_load.start()

    def partner(step):
        if n & (n - 1):
            return lax.rem(me + step, n)
        other, bit = 0, 1
        while bit < n:
            digit = lax.rem(me // bit, 2)
            other += bit * (1 - digit if step & bit else digit)
            bit *= 2
        return other

    partners = [partner(step) for step in range(n)]

    def send_to(phase, src, dst, peer, peer_core):
        pltpu.make_async_remote_copy(
            src_ref=src,
            dst_ref=dst,
            send_sem=r.send_sem.at[phase],
            recv_sem=r.recv_sem.at[phase],
            device_id=(peer, peer_core),
            device_id_type=MESH,
        ).start()

    def all_to_all(phase, send, recv, slot, same=False):
        for step in reversed(range(1, n)):
            peer = partners[step]
            src = send if same else send.at[pl.ds(pl.multiple_of(peer * slot, slot), slot)]
            send_to(
                phase, src, recv.at[pl.ds(pl.multiple_of(me * slot, slot), slot)], peer, core
            )

    def drain(sem, buffer, count):
        part = buffer.at[pl.ds(0, count)]
        pltpu.make_async_copy(part, part, sem).wait()

    def take(phase, send, recv, slot, same=False):
        drain(r.recv_sem.at[phase], recv, (n - 1) * slot)
        mine = pl.ds(pl.multiple_of(me * slot, slot), slot)
        recv[mine, :] = send[...] if same else send[mine, :]

    for load in small_loads:
        load.wait()
    x = r.tokens[...].astype(F32)
    normed = rms_scale(x, r.first_gain[...]).astype(BF16).astype(F32)
    for e in range(n):
        r.send1[e] = normed[:, e * LANES : (e + 1) * LANES]
    pl.semaphore_wait(barrier, n * nc - 1)
    for step in reversed(range(1, n)):
        send_to(0, r.send1.at[partners[step]], r.recv1.at[me], partners[step], core)
    for load in (write_load, read_load, step_load, state_load, out_load):
        load.start()
    send0 = r.send0
    send0[...] = jnp.zeros_like(send0)
    chosen = r.routes[...].astype(F32)
    scores = r.route_logits[...].astype(F32)
    for e in range(n):
        at, cut = e * slot0, slice(e * LANES, (e + 1) * LANES)
        send0[at : at + q, :] = x[:, cut]
        send0[at + q : at + 2 * q, 0:topk] = chosen
        send0[at + 2 * q : at + 3 * q, 0:topk] = scores
    all_to_all(6, send0, r.recv0, slot0)
    own = r.own_rows
    own[...] = jnp.zeros_like(own)
    own[0:q, :] = normed
    own_b = own[...].astype(BF16)
    gate_load.wait()
    inner_load.wait()

    drain(r.recv_sem.at[0], r.recv1, n - 1)
    r.recv1[me] = r.send1[me]

    features = jnp.concatenate([r.recv1[:, s, :] for s in range(q)], axis=0).astype(BF16)
    pack2 = r.pack2
    for g, weight in enumerate((r.gate_v, r.inner_v)):
        part = dot(features, weight[...])
        for s in range(q):
            for j in range(chunks):
                pack2[pl.ds((s * 2 + g) * chunks + j, n, stride=slot2), :] = part[
                    s * n : (s + 1) * n, j * LANES : (j + 1) * LANES
                ]
    r.send2[...] = pack2[...].astype(BF16)
    all_to_all(1, r.send2, r.recv2, slot2)

    for load in loads[7:]:
        load.start()
    write_load.wait()
    read_load.wait()
    step_load.wait()
    write_proj = dot(own_b, r.write_v[...])[0:q].astype(BF16)
    read_proj = dot(own_b, r.read_v[...])[0:q].astype(BF16)
    step_raw = lax.dot_general(
        own_b, r.step_v[...], (((1,), (1,)), ((), ())), preferred_element_type=F32
    )[0:q]
    gs = groups * state_width
    taps = r.conv_kernel.shape[0]
    for s in range(q):
        fresh = r.fresh
        fresh[0:1, :] = write_proj[s : s + 1].astype(F32)
        fresh[1:2, :] = read_proj[s : s + 1].astype(F32)
        newest = fresh[0:2, :]
        r.proj_out[s, taps - 2] = newest.astype(BF16)
        window = newest * r.conv_proj_kernel[taps - 1]
        for j in range(taps - 1):
            held = r.conv_proj_state[s, j]
            if j > 0:
                r.proj_out[s, j - 1] = held
            window += held.astype(F32) * r.conv_proj_kernel[j]
        window = silu(window)
        r.vectors[s : s + 1, 0:gs] = window[0:1]
        r.vectors[s : s + 1, gs:] = window[1:2]
    write, read = r.vectors[0:q, 0:gs], r.vectors[0:q, gs:]
    inner_part = jnp.zeros((q, half), F32)
    for j in range(taps - 1):
        held = r.conv_state[j]
        if j > 0:
            r.conv_out[j - 1] = held
        inner_part += held.astype(F32) * r.conv_kernel[j : j + 1, :]
    pre = step_raw + r.step_bias[...]
    step_size = jnp.maximum(pre, 0.0) + jnp.log1p(jnp.exp(-jnp.abs(pre)))
    decay = jnp.exp(-jnp.exp(r.log_rate[...]) * step_size)
    small = r.small
    small[...] = jnp.zeros_like(small)
    small[0:q, :] = step_size
    small[q : 2 * q, :] = decay
    small[2 * q : 2 * q + 1, :] = r.skip_gain[...]
    spread = (
        lax.broadcasted_iota(jnp.int32, (heads, half), 1) // head_width
        == lax.broadcasted_iota(jnp.int32, (heads, half), 0)
    ).astype(F32)
    by_channel = jnp.dot(small[...], spread, precision=highest, preferred_element_type=F32)
    step_rows, decay_rows = by_channel[0:q], by_channel[q : 2 * q]
    skip_rows = by_channel[2 * q : 2 * q + 1]
    reads = r.reads
    reads[...] = jnp.zeros_like(reads)
    reads[0:q, :] = read
    state_load.wait()
    old_read = r.old_read
    write_read = []
    for g in range(groups):
        lane = slice(g * state_width, (g + 1) * state_width)
        span = slice(g * group_width, (g + 1) * group_width)
        write_read.append(
            jnp.broadcast_to(
                jnp.sum(write[:, lane] * read[:, lane], axis=1, keepdims=True), (q, group_width)
            )
        )
        for s in range(q):
            old_read[s : s + 1, span] = lax.dot_general(
                reads[:, lane],
                r.hs[s, span, :],
                (((1,), (1,)), ((), ())),
                precision=highest,
                preferred_element_type=F32,
            )[s : s + 1]
    carried = decay_rows * old_read[0:q, :]
    direct = step_rows * jnp.concatenate(write_read, axis=1) + skip_rows

    take(1, r.send2, r.recv2, slot2)
    total = r.recv2[0:slot2, :].astype(F32)
    for e in range(1, n):
        total += r.recv2[e * slot2 : (e + 1) * slot2, :].astype(F32)
    r.sum2[...] = total
    gate_proj = lanes_of(r.sum2, 0, q, 2 * chunks, chunks).astype(BF16).astype(F32)
    inner_proj = lanes_of(r.sum2, chunks, q, 2 * chunks, chunks).astype(BF16)
    conv_inner = silu(inner_part + inner_proj.astype(F32) * r.conv_kernel[taps - 1 : taps, :])
    gated = (carried + direct * conv_inner) * silu(gate_proj)
    normal = []
    for g in range(groups):
        piece = gated[:, g * group_width : (g + 1) * group_width]
        normal.append(
            piece * lax.rsqrt(jnp.mean(piece * piece, axis=1, keepdims=True) + norm_eps)
        )
    mixer = jnp.concatenate(normal, axis=1) * r.group_gain[...]
    for j in range(chunks):
        r.pack3[pl.ds(j, q, stride=chunks), :] = mixer[:, j * LANES : (j + 1) * LANES]
    r.send3[...] = r.pack3[...].astype(BF16)
    all_to_all(2, r.send3, r.recv3, slot3, same=True)

    r.conv_out[taps - 2] = inner_proj
    turn = r.turn
    turn[...] = jnp.zeros_like(turn)
    turn[0:q, :] = decay_rows
    turn[q : 2 * q, :] = step_rows * conv_inner
    columns = jnp.transpose(turn[...])
    for s in range(q):
        for k in range(chunks):
            span = slice(k * LANES, (k + 1) * LANES)
            g = k * LANES // group_width
            r.state_out[s, span, :] = (
                columns[span, s : s + 1] * r.hs[s, span, :]
                + columns[span, q + s : q + s + 1]
                * write[s : s + 1, g * state_width : (g + 1) * state_width]
            )
    take(6, send0, r.recv0, slot0)

    def gathered(offset):
        return jnp.concatenate(
            [r.recv0[pl.ds(offset + s, n, stride=slot0), :] for s in range(q)], axis=0
        )

    raw_block = gathered(0)
    all_routes, all_scores = gathered(q), gathered(2 * q)
    real = lax.broadcasted_iota(jnp.int32, (rows, LANES), 1) < topk
    top = jnp.max(jnp.where(real, all_scores, -jnp.inf), axis=1, keepdims=True)
    raised = jnp.where(real, jnp.exp(jnp.where(real, all_scores - top, 0.0)), 0.0)
    gates = raised / jnp.sum(raised, axis=1, keepdims=True)
    hits = real & (all_routes == me.astype(F32))
    row_weight = jnp.sum(jnp.where(hits, gates, 0.0), axis=1, keepdims=True)
    out_load.wait()

    take(2, r.send3, r.recv3, slot3, same=True)
    r.wide3[...] = r.recv3[...].astype(F32)
    all_mixer = jnp.concatenate(
        [lanes_of(r.wide3, s * chunks, n, slot3, chunks) for s in range(q)], axis=0
    ).astype(BF16)
    part = dot(all_mixer, r.out_v[...])
    r.send4[...] = part
    swap = pltpu.make_async_remote_copy(
        src_ref=r.send4,
        dst_ref=r.recv4,
        send_sem=r.send_sem.at[3],
        recv_sem=r.recv_sem.at[3],
        device_id=(me, lax.rem(core + 1, nc)),
        device_id_type=MESH,
    )
    swap.start()
    swap.wait_recv()
    r.send5[...] = (raw_block + (part + r.recv4[...])).astype(BF16)
    all_to_all(4, r.send5, r.recv5, rows, same=True)
    expert_gate_load.wait()
    expert_up_load.wait()
    dense_up_load.wait()
    take(4, r.send5, r.recv5, rows, same=True)
    hidden = jnp.concatenate(
        [r.recv5[e * rows : (e + 1) * rows, :] for e in range(n)], axis=1
    ).astype(F32)
    r.hidden[...] = hidden
    mid = rms_scale(hidden, r.second_gain[...]).astype(BF16)
    dense_inner = silu(dot(mid, r.du_v[...])).astype(BF16)
    activated = clamped_unit(dot(mid, r.eg_v[...]), dot(mid, r.eu_v[...])).astype(BF16)
    dense_weight = jax.nn.sigmoid(
        jnp.sum(mid.astype(F32) * r.dense_gate[...], axis=1, keepdims=True)
    )
    expert_down_load.wait()
    dense_down_load.wait()
    cuts = 4
    for c in range(cuts):
        span = slice(c * width // cuts, (c + 1) * width // cuts)
        term = dot(activated, r.ed_v[:, span]) * row_weight
        term += dot(dense_inner, r.dd_v[:, span]) * dense_weight
        for j in range(wide_chunks // cuts):
            r.pack6[pl.ds(c * wide_chunks // cuts + j, rows, stride=slot6), :] = term[
                :, j * LANES : (j + 1) * LANES
            ]
    r.send6[...] = r.pack6[...].astype(BF16)
    mine = me * nc + core

    into = r.recv6.at[pl.ds(pl.multiple_of(mine * slot6, slot6), slot6)]
    for step in reversed(range(n)):
        for turn_core in range(1 if step == 0 else 0, nc):
            peer, peer_core = partners[step], lax.rem(core + turn_core, nc)
            row = pl.multiple_of((peer_core * n + peer) * slot6, slot6)
            send_to(5, r.send6.at[pl.ds(row, slot6)], into, peer, peer_core)
    own_row = r.hidden[pl.ds(core * n + me, 1), :]
    drain(r.recv_sem.at[5], r.recv6, (n * nc - 1) * slot6)
    r.recv6[pl.ds(pl.multiple_of(mine * slot6, slot6), slot6), :] = r.send6[
        pl.ds(pl.multiple_of((core * n + me) * slot6, slot6), slot6), :
    ]
    total = r.recv6[0:slot6, :].astype(F32)
    for e in range(1, n * nc):
        total += r.recv6[e * slot6 : (e + 1) * slot6, :].astype(F32)
    r.sum6[...] = total
    summed = jnp.concatenate([r.sum6[j : j + 1, :] for j in range(wide_chunks)], axis=1)
    r.layer_out[...] = (own_row + summed).astype(BF16)

    drain(r.send_sem.at[0], r.send1, n - 1)
    drain(r.send_sem.at[6], send0, (n - 1) * slot0)
    drain(r.send_sem.at[1], r.send2, (n - 1) * slot2)
    drain(r.send_sem.at[2], r.recv3, (n - 1) * slot3)
    swap.wait_send()
    drain(r.send_sem.at[4], r.recv5, (n - 1) * rows)
    drain(r.send_sem.at[5], r.send6, (n * nc - 1) * slot6)


def store_kernel(*refs):
    count = len(refs) // 2
    copies = [
        pltpu.make_async_copy(refs[i], refs[count + i], refs[-1].at[i]) for i in range(count)
    ]
    for copy in copies:
        copy.start()
    for copy in copies:
        copy.wait()


def fused_local(
    n,
    nc,
    tokens,
    head_state,
    conv_state,
    conv_proj_state,
    first_gain,
    gate_weight,
    inner_weight,
    write_weight,
    read_weight,
    step_weight,
    conv_kernel,
    conv_proj_kernel,
    step_bias,
    log_rate,
    skip_gain,
    group_gain,
    out_weight,
    second_gain,
    routes,
    route_logits,
    expert_gate,
    expert_up,
    expert_down,
    dense_up,
    dense_down,
    dense_gate,
):
    q, width = tokens.shape
    half = gate_weight.shape[1]
    rows = n * q
    chunks, wide_chunks = half // LANES, width // LANES
    gs = write_weight.shape[1]
    heads, state_width = head_state.shape[1], head_state.shape[3]
    taps = conv_kernel.shape[0]
    small_in = dict(
        tokens=tokens,
        first_gain=first_gain[None],
        conv_state=jnp.transpose(conv_state, (1, 0, 2)),
        conv_proj_state=conv_proj_state,
        conv_kernel=conv_kernel,
        conv_proj_kernel=conv_proj_kernel,
        step_bias=step_bias[None],
        log_rate=log_rate[None],
        skip_gain=skip_gain[None],
        group_gain=group_gain[None],
        second_gain=second_gain[None],
        routes=routes,
        route_logits=route_logits,
        dense_gate=dense_gate[None],
    )
    big_in = dict(
        head_state=head_state.reshape(q, half, state_width),
        gate_weight=gate_weight,
        inner_weight=inner_weight,
        write_weight=write_weight,
        read_weight=read_weight,
        step_weight=step_weight.T,
        out_weight=out_weight,
        expert_gate=expert_gate[0],
        expert_up=expert_up[0],
        expert_down=expert_down[0],
        dense_up=dense_up,
        dense_down=dense_down,
    )
    vmem = pltpu.VMEM
    outs = dict(
        layer_out=vmem((q // nc, width), BF16),
        state_out=vmem((q, half, state_width), F32),
        conv_out=vmem((taps - 1, q, half), BF16),
        proj_out=vmem((q, taps - 1, 2, gs), BF16),
    )
    slot0 = -(-3 * q // 8) * 8
    slot2, slot3, slot6 = 2 * q * chunks, q * chunks, wide_chunks
    small_rows = -(-(2 * q + 1) // 8) * 8
    scratch = dict(
        gate_v=vmem(gate_weight.shape, BF16),
        inner_v=vmem(inner_weight.shape, BF16),
        write_v=vmem(write_weight.shape, BF16),
        read_v=vmem(read_weight.shape, BF16),
        step_v=vmem(step_weight.shape[::-1], BF16),
        hs=vmem((q, half, state_width), F32),
        out_v=vmem(out_weight.shape, BF16),
        eg_v=vmem(expert_gate.shape[1:], BF16),
        eu_v=vmem(expert_up.shape[1:], BF16),
        du_v=vmem(dense_up.shape, BF16),
        ed_v=vmem(expert_down.shape[1:], BF16),
        dd_v=vmem(dense_down.shape, BF16),
        send0=vmem((n * slot0, LANES), F32),
        recv0=vmem((n * slot0, LANES), F32),
        send1=vmem((n, q, LANES), F32),
        recv1=vmem((n, q, LANES), F32),
        own_rows=vmem((16, width), F32),
        pack2=vmem((n * slot2, LANES), F32),
        send2=vmem((n * slot2, LANES), BF16),
        recv2=vmem((n * slot2, LANES), BF16),
        sum2=vmem((slot2, LANES), F32),
        fresh=vmem((8, gs), F32),
        vectors=vmem((8, 2 * gs), F32),
        small=vmem((small_rows, heads), F32),
        reads=vmem((8, gs), F32),
        old_read=vmem((8, half), F32),
        pack3=vmem((slot3, LANES), F32),
        send3=vmem((slot3, LANES), BF16),
        recv3=vmem((n * slot3, LANES), BF16),
        wide3=vmem((n * slot3, LANES), F32),
        turn=vmem((8, half), F32),
        send4=vmem((rows, LANES), F32),
        recv4=vmem((rows, LANES), F32),
        send5=vmem((rows, LANES), BF16),
        recv5=vmem((n * rows, LANES), BF16),
        hidden=vmem((rows, width), F32),
        pack6=vmem((rows * slot6, LANES), F32),
        send6=vmem((rows * slot6, LANES), BF16),
        recv6=vmem((n * nc * slot6, LANES), BF16),
        sum6=vmem((slot6, LANES), F32),
        load_sem=pltpu.SemaphoreType.DMA((12,)),
        small_sem=pltpu.SemaphoreType.DMA((len(small_in),)),
        send_sem=pltpu.SemaphoreType.DMA((7,)),
        recv_sem=pltpu.SemaphoreType.DMA((7,)),
    )
    in_vmem = pl.BlockSpec(memory_space=pltpu.VMEM)
    anywhere = pl.BlockSpec(memory_space=pl.ANY)
    names = tuple(big_in) + tuple(outs)
    results = pl.pallas_call(
        functools.partial(layer_kernel, n, nc, tuple(small_in), names, tuple(scratch)),
        out_shape=tuple(outs.values()),
        in_specs=[anywhere] * (len(small_in) + len(big_in)),
        out_specs=(in_vmem,) * len(outs),
        scratch_shapes=list(scratch.values())
        + [vmem(a.shape, a.dtype) for a in small_in.values()],
        compiler_params=pltpu.CompilerParams(
            collective_id=0, has_side_effects=True, vmem_limit_bytes=60 * 1024 * 1024
        ),
    )(*small_in.values(), *big_in.values())
    layer_out, state_out, conv_out, proj_out = pl.pallas_call(
        store_kernel,
        out_shape=tuple(jax.ShapeDtypeStruct(a.shape, a.dtype) for a in results),
        in_specs=[in_vmem] * len(results),
        out_specs=(anywhere,) * len(results),
        scratch_shapes=[pltpu.SemaphoreType.DMA((len(results),))],
    )(*[pltpu.with_memory_space_constraint(a, pltpu.VMEM) for a in results])
    return (
        layer_out,
        state_out.reshape(head_state.shape),
        jnp.transpose(conv_out, (1, 0, 2)),
        proj_out,
    )


def solution(mesh):
    n, nc = mesh.shape["ep"], mesh.shape["tp"]
    placed = (
        P("ep", None),
        P("ep", "tp", None, None),
        P("ep", None, "tp"),
        P("ep", None, None, "tp"),
        P(),
        P("ep", "tp"),
        P("ep", "tp"),
        P(None, "tp"),
        P(None, "tp"),
        P(None, "tp"),
        P(None, "tp"),
        P(None, None, "tp"),
        P("tp"),
        P("tp"),
        P("tp"),
        P("tp"),
        P("tp", "ep"),
        P(),
        P("ep", None),
        P("ep", None),
        P("ep", None, "tp"),
        P("ep", None, "tp"),
        P("ep", "tp", None),
        P(None, ("ep", "tp")),
        P(("ep", "tp"), None),
        P(),
    )

    def body(*args):
        seq, width = args[0].shape
        if width == n * LANES and seq == nc and args[5].shape[1] % LANES == 0:
            return fused_local(n, nc, *args)
        return local(*args)

    return jax.shard_map(
        body,
        mesh=mesh,
        in_specs=placed,
        out_specs=(
            P(("ep", "tp"), None),
            P("ep", "tp", None, None),
            P("ep", None, "tp"),
            P("ep", None, None, "tp"),
        ),
        check_vma=False,
    )
```
